32 devices in a mesh: fs: 16 (over z, y, x), tp: 2 (over core).
Axes of the slice: x: 2, y: 2, z: 4, core: 2. Of those that a mesh axis runs over, the one named last changes fastest.
Arguments:
- late_input: bfloat16 [2048, 2048], P('fs', 'tp'), may hold values from -6 to 6
- up_weight: bfloat16 [2048, 4096], P('tp', 'fs'), may hold values from -0.125 to 0.125
- down_weight: bfloat16 [4096, 2048], P('fs', 'tp'), may hold values from -0.09375 to 0.09375
- early_input: bfloat16 [2048, 2048], P('fs', 'tp'), may hold values from -6 to 6
- early_pre: bfloat16 [2048, 4096], P('fs'), may hold values from -6 to 6
- cotangent: bfloat16 [2048, 2048], P('fs', 'tp'), may hold values from -6 to 6
- up_sum: float32 [2048, 4096], P('tp', 'fs'), may hold values from -24 to 24
- down_sum: float32 [4096, 2048], P('fs', 'tp'), may hold values from -24 to 24
Outputs:
- late_pre: bfloat16 [2048, 4096], P('fs')
- late_out: bfloat16 [2048, 2048], P('fs', 'tp')
- input_grad: bfloat16 [2048, 2048], P('fs', 'tp')
- up_total: float32 [2048, 4096], P('tp', 'fs')
- down_total: float32 [4096, 2048], P('fs', 'tp')
The draws below stay inside these ranges and needn't reach their ends.
All inputs are finite; a program needn't handle non-finite values.
Results may differ from the reference program's by a relative error of at most 0.025.
Values may be sent and summed in bfloat16 or wider, within the bound.
A program may use at most 128 MiB of HBM per device.

```python
import jax
import jax.numpy as jnp
from jax import lax

D = 2048
FF = 4096
TOKENS = 2048
DBLK = 1024
N_TP = 2


def spiked(drawn, own_key, source, target, parts, factor):
    owner, partner = [(jnp.arange(drawn.shape[axis_at]) // (drawn.shape[axis_at] // parts)).reshape([-1 if axis == axis_at else 1 for axis in range(drawn.ndim)]) for axis_at in (source, target)]
    chosen = jax.random.permutation(own_key, parts)[partner]
    strong = (owner == chosen) | (owner == (partner + parts // 2) % parts)
    return jnp.where(strong, factor * drawn, drawn)


def steps_of(key, shape, split, smallest, largest):
    def one(position, shards_of):
        draws = jax.random.uniform(jax.random.fold_in(jax.random.fold_in(key, 6), position), (shards_of,), jnp.float32, smallest / len(split), largest / len(split))
        return jnp.repeat(jnp.exp(draws), shape[position] // shards_of).reshape((-1,) + (1,) * (len(shape) - position - 1))

    factor_of = one(*split[0])
    for cut in split[1:]:
        factor_of = factor_of * one(*cut)
    return factor_of


def centred(rng, shape, width, reach, split=(), held_as=jnp.bfloat16):
    loudness = steps_of(rng, shape, split, -0.22, 0.18) if split else 1.0
    values = jax.random.normal(rng, shape, jnp.float32) * width * loudness
    return jnp.minimum(jnp.maximum(values, -reach), reach).astype(held_as)


def bell_draw_with(key, shape, width, bound, pieces, heavy, held_as=jnp.bfloat16):
    values = width * jax.random.normal(key, shape, jnp.float32)
    if pieces:
        values = values * steps_of(key, shape, pieces, -0.22, 0.18)
    return jnp.clip(spiked(values, jax.random.fold_in(key, 3), *heavy), -bound, bound).astype(held_as)


def setup_inputs(seed: int = 0) -> dict:
    arg_keys = jax.random.split(jax.random.key(seed), 9)
    return {
        "late_input": centred(arg_keys[0], (TOKENS, D), 1.0, 6.0, ((0, 16), (1, 2))),
        "up_weight": centred(arg_keys[1], (D, FF), D ** -0.5, 0.125, ((0, 2), (1, 16))),
        "down_weight": centred(arg_keys[2], (FF, D), FF ** -0.5, 0.09375, ((0, 16), (1, 2))),
        "early_input": centred(arg_keys[3], (TOKENS, D), 1.0, 6.0, ((0, 16), (1, 2))),
        "early_pre": centred(arg_keys[4], (TOKENS, FF), 1.0, 6.0, ((0, 16),)),
        "cotangent": bell_draw_with(arg_keys[5], (TOKENS, D), 1.0, 6.0, ((0, 16), (1, 2)), (0, 1, 16, 2.0)),
        "up_sum": centred(arg_keys[6], (D, FF), 4.0, 24.0, ((0, 2), (1, 16)), jnp.float32),
        "down_sum": centred(arg_keys[7], (FF, D), 4.0, 24.0, ((0, 16), (1, 2)), jnp.float32),
    }


def block_sum(left, right):
    total = jnp.zeros((left.shape[0], right.shape[1]), jnp.float32)
    for block in range(N_TP):
        lower = block * DBLK
        partial_value = jnp.dot(left[:, lower:lower + DBLK], right[lower:lower + DBLK, :], preferred_element_type=jnp.float32)
        partial_value = lax.optimization_barrier(partial_value.astype(jnp.bfloat16))
        total = total + partial_value.astype(jnp.float32)
    return total


def reference(late_input, up_weight, down_weight, early_input, early_pre, cotangent, up_sum, down_sum):
    late_pre = block_sum(late_input, up_weight).astype(jnp.bfloat16)
    late_hidden = jnp.square(jax.nn.relu(late_pre.astype(jnp.float32))).astype(jnp.bfloat16)
    late_out = jnp.dot(late_hidden, down_weight, preferred_element_type=jnp.float32).astype(jnp.bfloat16)
    early_float = early_pre.astype(jnp.float32)
    early_hidden = jnp.square(jax.nn.relu(early_float)).astype(jnp.bfloat16)
    hidden_grad = block_sum(cotangent, down_weight.T)
    pre_grad = (hidden_grad * 2.0 * jax.nn.relu(early_float)).astype(jnp.bfloat16)
    input_grad = jnp.dot(pre_grad, up_weight.T, preferred_element_type=jnp.float32).astype(jnp.bfloat16)
    up_total = up_sum + jnp.dot(early_input.T, pre_grad, preferred_element_type=jnp.float32)
    down_total = down_sum + jnp.dot(early_hidden.T, cotangent, preferred_element_type=jnp.float32)
    return late_pre, late_out, input_grad, up_total, down_total
```

```python
import jax
import jax.numpy as jnp
from jax import lax
from jax.experimental import pallas as pl
from jax.experimental.pallas import tpu as pltpu
from jax.sharding import PartitionSpec as P

MESH = pl.DeviceIdType.MESH
F32 = jnp.float32
BF16 = jnp.bfloat16


def dot(left, right, lc, rc):
    return lax.dot_general(left, right, (((lc,), (rc,)), ((), ())), preferred_element_type=F32)


def square_relu(value):
    kept = jnp.maximum(value.astype(F32), 0.0)
    return (kept * kept).astype(BF16)


def fused(a, late_in, up_w, down_w, early_in, early_pre, cot,
          late_pre_o, late_out_o, in_grad_o, up_o, down_o,
          cot_g, late_g, early_g, pre_g, up_g, down_g, gt_s, gt_r, pg, eh, lt_s, lt_r, lp, lh, lp_g,
          part, ig_s, ig_u, ig_d, lo_s, lo_u, lo_d,
          dg_s, dg_x, dg_y, dg_fx, dg_fy, ug_s, ug_x, ug_y, ug_fx, ug_fy,
          ag_ss, ag_rs, w_ss, w_rs, e_ss, e_rs, l_ss, l_rs, t_ss, t_rs, rl_ss, rl_rs, rq_ss, rq_rs,
          local_s, down_v, up_v, ig_v, lo_v):
    side = 4
    half_side = side // 2
    me = lax.axis_index("fs")
    t = lax.axis_index("tp")
    z = me // side
    q = lax.rem(me, side)
    y = q // 2
    x = lax.rem(q, 2)
    qx = y * 2 + (1 - x)
    qy = (1 - y) * 2 + x
    qd = side - 1 - q
    xn = (z * side + qx, t)
    yn = (z * side + qy, t)
    pn = (me, 1 - t)
    above = (lax.rem(me + side, a * side), t)
    below = (lax.rem(me + (a - 1) * side, a * side), t)
    rows = late_in.shape[0]
    ff = up_w.shape[1]
    width = late_in.shape[1]
    cut = width // 2
    last = a - 1
    middle = (z > 0) & (z < last)

    def begin(src, dst, k):
        copy = pltpu.make_async_copy(src, dst, local_s.at[k])
        copy.start()
        return copy

    def slot(j):
        return pl.ds(pl.multiple_of(j * rows, rows), rows)

    def slots(n):
        size = rows // n
        return lambda j, c: pl.ds(pl.multiple_of(j * rows + c * size, size), size)

    def columns(block, unit):
        return pl.ds(pl.multiple_of(block * unit, unit), unit)

    own_rows = slot(z)
    own_down = begin(down_w, down_g.at[q], 0)
    own_cot = begin(cot, cot_g.at[own_rows], 1)
    own_late = begin(late_in, late_g.at[own_rows], 3)
    own_early = [begin(early_in.at[:, pl.ds(c * cut, cut)], early_g.at[c, own_rows], 14 + c) for c in range(2)]
    own_up = begin(up_w, up_g.at[q], 2)
    own_pre = [
        begin(early_pre.at[:, pl.ds(pl.multiple_of((z * side + b) * ff, ff), ff)],
              pre_g.at[b, own_rows], 5 + b)
        for b in range(side)
    ]

    barrier = pltpu.get_barrier_semaphore()
    greet = [xn, yn, pn] + [(lax.rem(me + o * side, a * side), t) for o in range(1, a)]
    for device in greet:
        pl.semaphore_signal(barrier, inc=1, device_id=device, device_id_type=MESH)
    pl.semaphore_wait(barrier, len(greet))

    sent = []

    def run(cond, go):
        if cond is None:
            go()
        else:
            pl.when(cond)(go)

    def rc(src, dst, ss, rs, device):
        return pltpu.make_async_remote_copy(
            src_ref=src, dst_ref=dst, send_sem=ss, recv_sem=rs, device_id=device, device_id_type=MESH)

    def send(src, dst, ss, rs, device, cond=None):
        copy = rc(src, dst, ss, rs, device)
        run(cond, copy.start)
        sent.append((cond, copy))

    def arrive(dst, ss, rs, cond=None):
        run(cond, rc(dst, dst, ss, rs, pn).wait_recv)

    gathers = {
        "cot": (0, 2, lambda j, c: cot_g.at[slots(2)(j, c)]),
        "late": (2, 2, lambda j, c: late_g.at[slots(2)(j, c)]),
        "early0": (4, 1, lambda j, c: early_g.at[0, slot(j)]),
        "early1": (5, 1, lambda j, c: early_g.at[1, slot(j)]),
    }

    def gather_own(name, depth=None):
        first, pieces, piece = gathers[name]
        for c in range(pieces):
            own = piece(z, c)
            for way, edge, device in ((0, z < last, above), (1, z > 0, below)):
                left = z if way == 0 else last - z
                cond = edge if depth is None else edge & (left == depth)
                send(own, own, ag_ss.at[first + c, way, 0], ag_rs.at[first + c, way, 1], device, cond)

    def gather_relay(name, d, some=None):
        if d >= last:
            return
        first, pieces, piece = gathers[name]
        for c in range(pieces) if some is None else some:
            for way, here, j, device in ((0, (z >= d) & (z < last), z - d, above),
                                         (1, (z + d < a) & (z > 0), z + d, below)):
                place = piece(jnp.clip(j, 0, last), c)
                arrive(place, ag_ss.at[first + c, way, 0], ag_rs.at[first + c, way, d], here)
                send(place, place, ag_ss.at[first + c, way, d], ag_rs.at[first + c, way, d + 1], device, here)

    def gather_end(name):
        first, pieces, piece = gathers[name]
        for d in range(1, a):
            for c in range(pieces):
                for way, here, j in ((0, z == last, z - d), (1, z == 0, z + d)):
                    place = piece(jnp.clip(j, 0, last), c)
                    arrive(place, ag_ss.at[first + c, way, 0], ag_rs.at[first + c, way, d], here)

    def half(ref, block, h):
        n = ref.shape[1] // 2
        return ref.at[block, pl.ds(h * n, n)]

    def half2(ref, h):
        n = ref.shape[0] // 2
        return ref.at[pl.ds(h * n, n)]

    def square_send(which, own, buf):
        for h in (0, 1):
            send(half2(own, h), half(buf, q, h), w_ss.at[which, 0, h], w_rs.at[which, 0, h], xn)
            send(half2(own, 1 - h), half(buf, q, 1 - h), w_ss.at[which, 1, 1 - h], w_rs.at[which, 1, 1 - h], yn)

    def square_relay(which, buf):
        arrive(half(buf, qx, 0), w_ss.at[which, 0, 0], w_rs.at[which, 0, 0])
        send(half(buf, qx, 0), half(buf, qx, 0), w_ss.at[which, 1, 2], w_rs.at[which, 1, 2], yn)
        arrive(half(buf, qy, 1), w_ss.at[which, 0, 0], w_rs.at[which, 1, 1])
        send(half(buf, qy, 1), half(buf, qy, 1), w_ss.at[which, 0, 2], w_rs.at[which, 0, 2], xn)

    def square_rest(which, buf):
        arrive(half(buf, qx, 1), w_ss.at[which, 0, 0], w_rs.at[which, 0, 1])
        arrive(half(buf, qy, 0), w_ss.at[which, 0, 0], w_rs.at[which, 1, 0])
        arrive(half(buf, qd, 0), w_ss.at[which, 0, 0], w_rs.at[which, 1, 2])
        arrive(half(buf, qd, 1), w_ss.at[which, 0, 0], w_rs.at[which, 0, 2])

    def square_sum(which, c, block, staged, first_x, first_y, fin_x, fin_y, out):
        n = staged.shape[1] // 2
        sems = lambda k: (rq_ss.at[which, c, k], rq_rs.at[which, c, k])
        wait = lambda dst, k: arrive(dst, *sems(k))

        def start():
            staged[qd] = block(qd).astype(BF16)
            send(half(staged, qd, 0), first_x, *sems(0), xn)
            send(half(staged, qd, 1), first_y, *sems(1), yn)
            staged[qx] = block(qx).astype(BF16)
            send(half(staged, qx, 0), half2(fin_x, 0), *sems(2), xn)
            staged[qy] = block(qy).astype(BF16)
            send(half(staged, qy, 1), half2(fin_y, 1), *sems(3), yn)

        def relay():
            wait(first_x, 0)
            staged[qy, 0:n] = (staged[qy, 0:n].astype(F32) + first_x[...].astype(F32)).astype(BF16)
            send(half(staged, qy, 0), half2(fin_y, 0), *sems(4), yn)
            wait(first_y, 1)
            staged[qx, n:2 * n] = (staged[qx, n:2 * n].astype(F32) + first_y[...].astype(F32)).astype(BF16)
            send(half(staged, qx, 1), half2(fin_x, 1), *sems(5), xn)

        def own():
            out[...] = block(q)

        def finish():
            wait(half2(fin_x, 0), 2)
            wait(half2(fin_y, 1), 3)
            wait(half2(fin_y, 0), 4)
            wait(half2(fin_x, 1), 5)
            out[...] = out[...] + (fin_x[...].astype(F32) + fin_y[...].astype(F32))

        return start, relay, own, finish

    def line_sum(which, c, value, staged, from_u, from_d, out):
        own = part.at[which, c]

        def go(way, j, step, cond):
            buf, device = ((from_u, above), (from_d, below))[way]
            send(staged.at[c, j], buf.at[c, j], rl_ss.at[which, c, way, step], rl_rs.at[which, c, way, j], device, cond)

        def start():
            own[...] = value(c)
            for j in range(a):
                staged[c, j] = own[pl.ds(j * rows, rows)].astype(BF16)
            for step in range(last):
                go(0, last - step, step, z == 0)
                go(1, step, step, z == last)

        def relay(step, opening):
            if step >= last:
                return
            for way in range(2):
                if way == 0:
                    j, on, opens, buf = last + z - step, step >= z, z == step, from_u
                else:
                    j, on, opens, buf = step - (last - z), step >= last - z, last - z == step, from_d
                on = on & middle & (opens if opening else jnp.logical_not(opens))
                j = jnp.clip(j, 0, last)

                @pl.when(on)
                def _(j=j, buf=buf, way=way):
                    arrive(buf.at[c, j], rl_ss.at[which, 0, 0, 0], rl_rs.at[which, c, way, j])
                    staged[c, j] = (staged[c, j].astype(F32) + buf[c, j].astype(F32)).astype(BF16)

                go(way, j, step, on)

        def finish():
            @pl.when(z > 0)
            def _():
                arrive(from_u.at[c, z], rl_ss.at[which, 0, 0, 0], rl_rs.at[which, c, 0, z])
                own[own_rows] = own[own_rows] + from_u[c, z].astype(F32)

            @pl.when(z < last)
            def _():
                arrive(from_d.at[c, z], rl_ss.at[which, 0, 0, 0], rl_rs.at[which, c, 1, z])
                own[own_rows] = own[own_rows] + from_d[c, z].astype(F32)

            out[:, pl.ds(c * cut, cut)] = own[own_rows].astype(BF16)

        return start, relay, finish

    def hops(b_of, go, offsets=None):
        for o in range(1, a) if offsets is None else offsets:
            if o < a:
                zs = lax.rem(z - o + a, a)
                for u in range(half_side):
                    go(o, u, zs, b_of(u))

    mine = lambda u: t * half_side + u
    other = lambda u: (1 - t) * half_side + u

    def pre_relay(o, u, zs, b):
        place = pre_g.at[b, slot(zs)]
        arrive(place, e_ss.at[0, 0, 0], e_rs.at[0, o, u])
        send(place, place, e_ss.at[1, o, u], e_rs.at[1, o, u], pn)

    def pre_rest(o, u, zs, b):
        arrive(pre_g.at[b, slot(zs)], e_ss.at[0, 0, 0], e_rs.at[1, o, u])

    def out_relay(o, u, zs, b):
        place = lp_g.at[:, columns(zs * side + b, ff)]
        arrive(place, l_ss.at[0, 0, 0], l_rs.at[0, o, u])
        send(place, place, l_ss.at[1, o, u], l_rs.at[1, o, u], pn)

    def out_rest(o, u, zs, b):
        arrive(lp_g.at[:, columns(zs * side + b, ff)], l_ss.at[0, 0, 0], l_rs.at[1, o, u])

    def ig_value(c):
        return sum(dot(pg[b], up_g[b, pl.ds(c * cut, cut), :], 1, 1) for b in range(side))

    def lo_value(c):
        return sum(dot(lh[b], down_g[b, :, pl.ds(c * cut, cut)], 1, 0) for b in range(side))

    ig = [line_sum(0, c, ig_value, ig_s, ig_u, ig_d, ig_v) for c in range(2)]
    lo = [line_sum(1, c, lo_value, lo_s, lo_u, lo_d, lo_v) for c in range(2)]
    dg = square_sum(1, 0, lambda b: dot(eh[b], cot_g[...], 0, 0), dg_s, dg_x, dg_y, dg_fx, dg_fy, down_v)
    ug = [
        square_sum(0, c, lambda b, c=c: dot(early_g[c], pg[b], 0, 0), ug_s.at[c], ug_x.at[c], ug_y.at[c],
                   ug_fx.at[c], ug_fy.at[c], up_v.at[pl.ds(c * cut, cut)])
        for c in range(2)
    ]

    own_down.wait()
    square_send(1, down_g.at[q], down_g)
    own_cot.wait()
    gather_own("cot")
    for o in range(1, a):
        zd = lax.rem(z + o, a)
        for u in range(half_side):
            b = mine(u)
            send(early_pre.at[:, columns(zd * side + b, ff)], pre_g.at[b, slot(z)],
                 e_ss.at[0, o, u], e_rs.at[0, o, u], (zd * side + q, t))
    own_late.wait()
    gather_own("late", 0)
    for copy in own_early:
        copy.wait()
    gather_own("early0", 0)
    gather_own("early1", 0)
    own_up.wait()
    for copy in own_pre:
        copy.wait()
    gather_relay("cot", 1)
    gather_own("late", 1)
    square_relay(1, down_g)
    square_send(0, up_g.at[q], up_g)
    for d in range(2, last):
        gather_relay("cot", d)
        gather_own("late", d)
    hops(mine, pre_relay, (1,))
    gather_relay("late", 1, (0,))
    gather_end("cot")
    square_rest(1, down_g)

    @pl.loop(0, side)
    def _(b):
        gt_s[b] = dot(cot_g[...], down_g[b], 1, 1).astype(BF16)

    send(gt_s, gt_r, t_ss.at[0], t_rs.at[0], pn)
    square_relay(0, up_g)
    hops(mine, pre_relay, range(2, a))
    gather_relay("late", 1, (1,))
    gather_own("early0", 1)
    gather_own("early1", 1)
    hops(other, pre_rest)

    @pl.loop(0, side)
    def _(b):
        eh[b] = square_relu(pre_g[b])

    arrive(gt_r, t_ss.at[0], t_rs.at[0])

    @pl.loop(0, side)
    def _(b):
        hidden = gt_s[b].astype(F32) + gt_r[b].astype(F32)
        pg[b] = (hidden * 2.0 * jnp.maximum(pre_g[b].astype(F32), 0.0)).astype(BF16)

    dg_start, dg_relay, dg_own, dg_finish = dg
    dg_start()
    gather_relay("early0", 1)
    square_rest(0, up_g)
    ig[0][0]()
    gather_relay("late", 2, (0,))
    ig[1][0]()
    dg_relay()
    gather_relay("late", 2, (1,))
    for d in range(3, last):
        gather_relay("late", d)
    for d in range(2, last):
        gather_own("early0", d)
        gather_own("early1", d)
    gather_relay("early1", 1)
    ig[0][1](1, True)
    gather_end("late")

    @pl.loop(0, side)
    def _(b):
        lt_s[b] = dot(late_g[...], up_g[b], 1, 0).astype(BF16)

    send(lt_s, lt_r, t_ss.at[1], t_rs.at[1], pn)
    ig[0][1](2, False)
    for d in range(2, last):
        gather_relay("early0", d)
    arrive(lt_r, t_ss.at[1], t_rs.at[1])

    @pl.loop(0, side)
    def _(b):
        pre = (lt_s[b].astype(F32) + lt_r[b].astype(F32)).astype(BF16)
        lp[b] = pre
        lh[b] = square_relu(pre)

    lo[0][0]()
    lo[1][0]()
    for o in range(1, a):
        zd = lax.rem(z + o, a)
        for u in range(half_side):
            b = mine(u)
            send(lp.at[b, slot(zd)], lp_g.at[:, columns(z * side + b, ff)],
                 l_ss.at[0, o, u], l_rs.at[0, o, u], (zd * side + q, t))
    ig[1][1](1, True)
    for d in range(2, last):
        gather_relay("early1", d)
    gather_end("early0")
    ug[0][0]()
    ig[1][1](2, False)
    ig[0][1](2, True)
    lo[0][1](1, True)
    dg_own()
    dg_finish()
    out_down = begin(down_v, down_o, 9)
    ug[0][1]()
    ig[1][1](2, True)
    for k in range(3, last):
        for c in range(2):
            for opening in (False, True):
                ig[c][1](k, opening)
    gather_end("early1")
    ug[1][0]()
    lo[0][1](2, False)
    lo[0][1](2, True)
    lo[1][1](1, True)
    ug[1][1]()
    ig[0][2]()
    ig[1][2]()
    out_ig = begin(ig_v, in_grad_o, 10)
    lo[1][1](2, False)
    lo[1][1](2, True)
    for k in range(3, last):
        for c in range(2):
            for opening in (False, True):
                lo[c][1](k, opening)
    for b in range(side):
        lp_g[:, columns(z * side + b, ff)] = lp[b, slot(z)]
    ug[0][2]()
    ug[1][2]()
    hops(mine, out_relay)
    ug[0][3]()
    lo[0][2]()
    ug[1][3]()
    out_up = begin(up_v, up_o, 13)
    lo[1][2]()
    out_lo = begin(lo_v, late_out_o, 12)
    hops(other, out_rest)
    out_pre = begin(lp_g, late_pre_o, 11)

    for cond, copy in sent:
        run(cond, copy.wait_send)
    for copy in (out_down, out_ig, out_pre, out_lo, out_up):
        copy.wait()


def fused_body(late_input, up_weight, down_weight, early_input, early_pre, cotangent, up_sum, down_sum):
    a = lax.axis_size("fs") // 4
    side = 4
    rows, width = late_input.shape
    ff = up_weight.shape[1]
    tokens, hidden = rows * a, ff * side
    cut = width // 2
    V = pltpu.VMEM
    D = pltpu.SemaphoreType.DMA
    token_block = V((tokens, width), BF16)
    hidden_block = V((side, tokens, ff), BF16)
    line_block = V((2, a, rows, cut), BF16)
    scratch = (
        [token_block] * 2
        + [V((2, tokens, cut), BF16)]
        + [hidden_block, V((side, width, ff), BF16), V((side, ff, width), BF16)]
        + [hidden_block] * 8
        + [V((rows, hidden * a), BF16), V((2, 2, tokens, cut), F32)]
        + [line_block] * 6
        + [V((side, ff, width), BF16)] + [V((ff // 2, width), BF16)] * 2 + [V((ff, width), BF16)] * 2
        + [V((2, side, cut, ff), BF16)] + [V((2, cut // 2, ff), BF16)] * 2 + [V((2, cut, ff), BF16)] * 2
        + [D((6, 2, a)), D((6, 2, a)), D((2, 2, 3)), D((2, 2, 3)), D((2, a, 2)), D((2, a, 2)),
           D((2, a, 2)), D((2, a, 2)), D((2,)), D((2,)), D((2, 2, 2, a)), D((2, 2, 2, a)),
           D((2, 2, 6)), D((2, 2, 6)), D((16,))]
        + [V((ff, width), F32), V((width, ff), F32)] + [V((rows, width), BF16)] * 2
    )
    flops = 12 * tokens * hidden * width
    late_pre, late_out, input_grad, up_grad, down_grad = pl.pallas_call(
        lambda *refs: fused(a, *refs),
        out_shape=(
            jax.ShapeDtypeStruct(early_pre.shape, BF16),
            jax.ShapeDtypeStruct(late_input.shape, BF16),
            jax.ShapeDtypeStruct(early_input.shape, BF16),
            jax.ShapeDtypeStruct(up_sum.shape, F32),
            jax.ShapeDtypeStruct(down_sum.shape, F32),
        ),
        in_specs=[pl.BlockSpec(memory_space=pl.ANY)] * 6,
        out_specs=[pl.BlockSpec(memory_space=pl.ANY)] * 5,
        scratch_shapes=scratch,
        compiler_params=pltpu.CompilerParams(
            collective_id=0, has_side_effects=True, vmem_limit_bytes=62 * 1024 * 1024),
        cost_estimate=pl.CostEstimate(flops=flops, bytes_accessed=1 << 24, transcendentals=0),
    )(late_input, up_weight, down_weight, early_input, early_pre, cotangent)
    return late_pre, late_out, input_grad, up_sum + up_grad, down_sum + down_grad


def contract_rows(left, right):
    return lax.dot_general(
        left, right, (((0,), (0,)), ((), ())), preferred_element_type=jnp.float32
    )


def contract_cols(left, right):
    return lax.dot_general(
        left, right, (((1,), (1,)), ((), ())), preferred_element_type=jnp.float32
    )


def body(late_input, up_weight, down_weight, early_input, early_pre, cotangent, up_sum, down_sum):
    up_gathered = lax.all_gather(up_weight, "fs", axis=1, tiled=True)
    down_gathered = lax.all_gather(down_weight, "fs", axis=0, tiled=True)
    pre_terms = jnp.dot(late_input, up_gathered, preferred_element_type=jnp.float32)
    pre_summed = lax.psum(pre_terms.astype(jnp.bfloat16), "tp")
    late_hidden = jnp.square(jax.nn.relu(pre_summed.astype(jnp.float32))).astype(jnp.bfloat16)
    early_float = early_pre.astype(jnp.float32)
    early_hidden = jnp.square(jax.nn.relu(early_float)).astype(jnp.bfloat16)
    late_out = jnp.dot(late_hidden, down_gathered, preferred_element_type=jnp.float32).astype(
        jnp.bfloat16
    )
    grad_terms = contract_cols(cotangent, down_gathered)
    hidden_grad = lax.psum(grad_terms.astype(jnp.bfloat16), "tp").astype(jnp.float32)
    pre_grad = (hidden_grad * 2.0 * jax.nn.relu(early_float)).astype(jnp.bfloat16)
    input_grad = contract_cols(pre_grad, up_gathered).astype(jnp.bfloat16)
    grad_local, hidden_local = (
        lax.all_to_all(pre_grad, "fs", split_axis=1, concat_axis=0, tiled=True),
        lax.all_to_all(early_hidden, "fs", split_axis=1, concat_axis=0, tiled=True),
    )
    rows = grad_local
    up_grad = contract_rows(lax.all_gather(early_input, "fs", axis=0, tiled=True), rows)
    up_total = up_sum + up_grad
    rows = hidden_local
    down_grad = contract_rows(rows, lax.all_gather(cotangent, "fs", axis=0, tiled=True))
    down_total = down_sum + down_grad
    return (pre_summed, late_out, input_grad, up_total, down_total)


def solution(mesh):
    in_specs = (
        P("fs", "tp"),
        P("tp", "fs"),
        P("fs", "tp"),
        P("fs", "tp"),
        P("fs", None),
        P("fs", "tp"),
        P("tp", "fs"),
        P("fs", "tp"),
    )
    out_specs = (P("fs", None), P("fs", "tp"), P("fs", "tp"), P("tp", "fs"), P("fs", "tp"))
    square_chips = mesh.shape["tp"] == 2 and mesh.shape["fs"] % 4 == 0 and mesh.shape["fs"] >= 8
    chosen = fused_body if square_chips else body
    return jax.shard_map(chosen, mesh=mesh, in_specs=in_specs, out_specs=out_specs, check_vma=False)
```

```python
import jax
import jax.numpy as jnp
from jax import lax
from jax.experimental import pallas as pl
from jax.experimental.pallas import tpu as pltpu
from jax.sharding import PartitionSpec as P

MESH = pl.DeviceIdType.MESH
F32 = jnp.float32
BF16 = jnp.bfloat16


def dot(left, right, lc, rc):
    return lax.dot_general(left, right, (((lc,), (rc,)), ((), ())), preferred_element_type=F32)


def square_relu(value):
    kept = jnp.maximum(value.astype(F32), 0.0)
    return (kept * kept).astype(BF16)


def fused(a, late_in, up_w, down_w, early_in, early_pre, cot, up_old, down_old,
          late_pre_o, lo_v, ig_v, up_v, down_v,
          cot_g, late_g, early_g, pre_g, up_g, down_g, gt_s, gt_r, pg, eh, lt_s, lt_r, lp, lh, lp_g,
          part, ig_s, ig_u, ig_d, lo_s, lo_u, lo_d,
          dg_s, dg_x, dg_y, dg_fx, dg_fy, ug_s, ug_x, ug_y, ug_fx, ug_fy,
          ag_ss, ag_rs, w_ss, w_rs, e_ss, e_rs, l_ss, l_rs, t_ss, t_rs, rl_ss, rl_rs, rq_ss, rq_rs,
          local_s, up_was, down_was):
    side = 4
    half_side = side // 2
    me = lax.axis_index("fs")
    t = lax.axis_index("tp")
    z = me // side
    q = lax.rem(me, side)
    y = q // 2
    x = lax.rem(q, 2)
    qx = y * 2 + (1 - x)
    qy = (1 - y) * 2 + x
    qd = side - 1 - q
    xn = (z * side + qx, t)
    yn = (z * side + qy, t)
    pn = (me, 1 - t)
    above = (lax.rem(me + side, a * side), t)
    below = (lax.rem(me + (a - 1) * side, a * side), t)
    rows = late_in.shape[0]
    ff = up_w.shape[1]
    width = late_in.shape[1]
    cut = width // 2
    last = a - 1
    middle = (z > 0) & (z < last)

    def begin(src, dst, k):
        copy = pltpu.make_async_copy(src, dst, local_s.at[k])
        copy.start()
        return copy

    def slot(j):
        return pl.ds(pl.multiple_of(j * rows, rows), rows)

    def slots(n):
        size = rows // n
        return lambda j, c: pl.ds(pl.multiple_of(j * rows + c * size, size), size)

    def columns(block, unit):
        return pl.ds(pl.multiple_of(block * unit, unit), unit)

    own_rows = slot(z)
    own_down = begin(down_w, down_g.at[q], 0)
    own_cot = begin(cot, cot_g.at[own_rows], 1)
    own_late = begin(late_in, late_g.at[own_rows], 3)
    own_early = [begin(early_in.at[:, pl.ds(c * cut, cut)], early_g.at[c, own_rows], 9 + c) for c in range(2)]
    own_up = begin(up_w, up_g.at[q], 2)
    own_pre = [
        begin(early_pre.at[:, pl.ds(pl.multiple_of((z * side + b) * ff, ff), ff)],
              pre_g.at[b, own_rows], 5 + b)
        for b in range(side)
    ]

    own_sums = [begin(up_old, up_was, 11), begin(down_old, down_was, 12)]

    barrier = pltpu.get_barrier_semaphore()
    greet = [xn, yn, pn] + [(lax.rem(me + o * side, a * side), t) for o in range(1, a)]
    for device in greet:
        pl.semaphore_signal(barrier, inc=1, device_id=device, device_id_type=MESH)
    pl.semaphore_wait(barrier, len(greet))

    sent = []

    def run(cond, go):
        if cond is None:
            go()
        else:
            pl.when(cond)(go)

    def rc(src, dst, ss, rs, device):
        return pltpu.make_async_remote_copy(
            src_ref=src, dst_ref=dst, send_sem=ss, recv_sem=rs, device_id=device, device_id_type=MESH)

    def send(src, dst, ss, rs, device, cond=None):
        copy = rc(src, dst, ss, rs, device)
        run(cond, copy.start)
        sent.append((cond, copy))

    def arrive(dst, ss, rs, cond=None):
        run(cond, rc(dst, dst, ss, rs, pn).wait_recv)

    gathers = {
        "cot": (0, 2, lambda j, c: cot_g.at[slots(2)(j, c)]),
        "late": (2, 2, lambda j, c: late_g.at[slots(2)(j, c)]),
        "early0": (4, 1, lambda j, c: early_g.at[0, slot(j)]),
        "early1": (5, 1, lambda j, c: early_g.at[1, slot(j)]),
    }

    def gather_own(name, depth=None):
        first, pieces, piece = gathers[name]
        for c in range(pieces):
            own = piece(z, c)
            for way, edge, device in ((0, z < last, above), (1, z > 0, below)):
                left = z if way == 0 else last - z
                cond = edge if depth is None else edge & (left == depth)
                send(own, own, ag_ss.at[first + c, way, 0], ag_rs.at[first + c, way, 1], device, cond)

    def gather_relay(name, d, some=None):
        if d >= last:
            return
        first, pieces, piece = gathers[name]
        for c in range(pieces) if some is None else some:
            for way, here, j, device in ((0, (z >= d) & (z < last), z - d, above),
                                         (1, (z + d < a) & (z > 0), z + d, below)):
                place = piece(jnp.clip(j, 0, last), c)
                arrive(place, ag_ss.at[first + c, way, 0], ag_rs.at[first + c, way, d], here)
                send(place, place, ag_ss.at[first + c, way, d], ag_rs.at[first + c, way, d + 1], device, here)

    def gather_end(name):
        first, pieces, piece = gathers[name]
        for d in range(1, a):
            for c in range(pieces):
                for way, here, j in ((0, z == last, z - d), (1, z == 0, z + d)):
                    place = piece(jnp.clip(j, 0, last), c)
                    arrive(place, ag_ss.at[first + c, way, 0], ag_rs.at[first + c, way, d], here)

    def half(ref, block, h):
        n = ref.shape[1] // 2
        return ref.at[block, pl.ds(h * n, n)]

    def half2(ref, h):
        n = ref.shape[0] // 2
        return ref.at[pl.ds(h * n, n)]

    def square_send(which, own, buf):
        for h in (0, 1):
            send(half2(own, h), half(buf, q, h), w_ss.at[which, 0, h], w_rs.at[which, 0, h], xn)
            send(half2(own, 1 - h), half(buf, q, 1 - h), w_ss.at[which, 1, 1 - h], w_rs.at[which, 1, 1 - h], yn)

    def square_relay(which, buf):
        arrive(half(buf, qx, 0), w_ss.at[which, 0, 0], w_rs.at[which, 0, 0])
        send(half(buf, qx, 0), half(buf, qx, 0), w_ss.at[which, 1, 2], w_rs.at[which, 1, 2], yn)
        arrive(half(buf, qy, 1), w_ss.at[which, 0, 0], w_rs.at[which, 1, 1])
        send(half(buf, qy, 1), half(buf, qy, 1), w_ss.at[which, 0, 2], w_rs.at[which, 0, 2], xn)

    def square_rest(which, buf):
        arrive(half(buf, qx, 1), w_ss.at[which, 0, 0], w_rs.at[which, 0, 1])
        arrive(half(buf, qy, 0), w_ss.at[which, 0, 0], w_rs.at[which, 1, 0])
        arrive(half(buf, qd, 0), w_ss.at[which, 0, 0], w_rs.at[which, 1, 2])
        arrive(half(buf, qd, 1), w_ss.at[which, 0, 0], w_rs.at[which, 0, 2])

    def square_sum(which, c, block, staged, first_x, first_y, fin_x, fin_y, was, out):
        n = staged.shape[1] // 2
        sems = lambda k: (rq_ss.at[which, c, k], rq_rs.at[which, c, k])
        wait = lambda dst, k: arrive(dst, *sems(k))

        def start():
            staged[qd] = block(qd).astype(BF16)
            send(half(staged, qd, 0), first_x, *sems(0), xn)
            send(half(staged, qd, 1), first_y, *sems(1), yn)
            staged[qx] = block(qx).astype(BF16)
            send(half(staged, qx, 0), half2(fin_x, 0), *sems(2), xn)
            staged[qy] = block(qy).astype(BF16)
            send(half(staged, qy, 1), half2(fin_y, 1), *sems(3), yn)

        def relay():
            wait(first_x, 0)
            staged[qy, 0:n] = (staged[qy, 0:n].astype(F32) + first_x[...].astype(F32)).astype(BF16)
            send(half(staged, qy, 0), half2(fin_y, 0), *sems(4), yn)
            wait(first_y, 1)
            staged[qx, n:2 * n] = (staged[qx, n:2 * n].astype(F32) + first_y[...].astype(F32)).astype(BF16)
            send(half(staged, qx, 1), half2(fin_x, 1), *sems(5), xn)

        def own():
            out[...] = block(q)

        def finish():
            wait(half2(fin_x, 0), 2)
            wait(half2(fin_y, 1), 3)
            wait(half2(fin_y, 0), 4)
            wait(half2(fin_x, 1), 5)
            out[...] = was[...] + (out[...] + (fin_x[...].astype(F32) + fin_y[...].astype(F32)))

        return start, relay, own, finish

    def line_sum(which, c, value, staged, from_u, from_d, out):
        own = part.at[which, c]

        def go(way, j, step, cond):
            buf, device = ((from_u, above), (from_d, below))[way]
            send(staged.at[c, j], buf.at[c, j], rl_ss.at[which, c, way, step], rl_rs.at[which, c, way, j], device, cond)

        def start():
            own[...] = value(c)
            for j in range(a):
                staged[c, j] = own[pl.ds(j * rows, rows)].astype(BF16)
            for step in range(last):
                go(0, last - step, step, z == 0)
                go(1, step, step, z == last)

        def relay(step, opening):
            if step >= last:
                return
            for way in range(2):
                if way == 0:
                    j, on, opens, buf = last + z - step, step >= z, z == step, from_u
                else:
                    j, on, opens, buf = step - (last - z), step >= last - z, last - z == step, from_d
                on = on & middle & (opens if opening else jnp.logical_not(opens))
                j = jnp.clip(j, 0, last)

                @pl.when(on)
                def _(j=j, buf=buf, way=way):
                    arrive(buf.at[c, j], rl_ss.at[which, 0, 0, 0], rl_rs.at[which, c, way, j])
                    staged[c, j] = (staged[c, j].astype(F32) + buf[c, j].astype(F32)).astype(BF16)

                go(way, j, step, on)

        def finish():
            @pl.when(z > 0)
            def _():
                arrive(from_u.at[c, z], rl_ss.at[which, 0, 0, 0], rl_rs.at[which, c, 0, z])
                own[own_rows] = own[own_rows] + from_u[c, z].astype(F32)

            @pl.when(z < last)
            def _():
                arrive(from_d.at[c, z], rl_ss.at[which, 0, 0, 0], rl_rs.at[which, c, 1, z])
                own[own_rows] = own[own_rows] + from_d[c, z].astype(F32)

            out[:, pl.ds(c * cut, cut)] = own[own_rows].astype(BF16)

        return start, relay, finish

    def hops(b_of, go, offsets=None):
        for o in range(1, a) if offsets is None else offsets:
            if o < a:
                zs = lax.rem(z - o + a, a)
                for u in range(half_side):
                    go(o, u, zs, b_of(u))

    mine = lambda u: t * half_side + u
    other = lambda u: (1 - t) * half_side + u

    def pre_relay(o, u, zs, b):
        place = pre_g.at[b, slot(zs)]
        arrive(place, e_ss.at[0, 0, 0], e_rs.at[0, o, u])
        send(place, place, e_ss.at[1, o, u], e_rs.at[1, o, u], pn)

    def pre_rest(o, u, zs, b):
        arrive(pre_g.at[b, slot(zs)], e_ss.at[0, 0, 0], e_rs.at[1, o, u])

    def out_relay(o, u, zs, b):
        place = lp_g.at[:, columns(zs * side + b, ff)]
        arrive(place, l_ss.at[0, 0, 0], l_rs.at[0, o, u])
        send(place, place, l_ss.at[1, o, u], l_rs.at[1, o, u], pn)

    def out_rest(o, u, zs, b):
        arrive(lp_g.at[:, columns(zs * side + b, ff)], l_ss.at[0, 0, 0], l_rs.at[1, o, u])

    def ig_value(c):
        return sum(dot(pg[b], up_g[b, pl.ds(c * cut, cut), :], 1, 1) for b in range(side))

    def lo_value(c):
        return sum(dot(lh[b], down_g[b, :, pl.ds(c * cut, cut)], 1, 0) for b in range(side))

    ig = [line_sum(0, c, ig_value, ig_s, ig_u, ig_d, ig_v) for c in range(2)]
    lo = [line_sum(1, c, lo_value, lo_s, lo_u, lo_d, lo_v) for c in range(2)]
    dg = square_sum(1, 0, lambda b: dot(eh[b], cot_g[...], 0, 0), dg_s, dg_x, dg_y, dg_fx, dg_fy, down_was, down_v)
    ug = [
        square_sum(0, c, lambda b, c=c: dot(early_g[c], pg[b], 0, 0), ug_s.at[c], ug_x.at[c], ug_y.at[c],
                   ug_fx.at[c], ug_fy.at[c], up_was.at[pl.ds(c * cut, cut)], up_v.at[pl.ds(c * cut, cut)])
        for c in range(2)
    ]

    own_down.wait()
    square_send(1, down_g.at[q], down_g)
    own_cot.wait()
    gather_own("cot")
    for o in range(1, a):
        zd = lax.rem(z + o, a)
        for u in range(half_side):
            b = mine(u)
            send(early_pre.at[:, columns(zd * side + b, ff)], pre_g.at[b, slot(z)],
                 e_ss.at[0, o, u], e_rs.at[0, o, u], (zd * side + q, t))
    own_late.wait()
    gather_own("late", 0)
    for copy in own_early:
        copy.wait()
    gather_own("early0", 0)
    gather_own("early1", 0)
    own_up.wait()
    for copy in own_pre:
        copy.wait()
    gather_relay("cot", 1)
    gather_own("late", 1)
    square_relay(1, down_g)
    square_send(0, up_g.at[q], up_g)
    for d in range(2, last):
        gather_relay("cot", d)
        gather_own("late", d)
    hops(mine, pre_relay, (1,))
    gather_relay("late", 1, (0,))
    gather_end("cot")
    square_rest(1, down_g)

    @pl.loop(0, side)
    def _(b):
        gt_s[b] = dot(cot_g[...], down_g[b], 1, 1).astype(BF16)

    send(gt_s, gt_r, t_ss.at[0], t_rs.at[0], pn)
    square_relay(0, up_g)
    hops(mine, pre_relay, range(2, a))
    gather_relay("late", 1, (1,))
    gather_own("early0", 1)
    gather_own("early1", 1)
    hops(other, pre_rest)

    @pl.loop(0, side)
    def _(b):
        eh[b] = square_relu(pre_g[b])

    arrive(gt_r, t_ss.at[0], t_rs.at[0])

    @pl.loop(0, side)
    def _(b):
        hidden = gt_s[b].astype(F32) + gt_r[b].astype(F32)
        pg[b] = (hidden * 2.0 * jnp.maximum(pre_g[b].astype(F32), 0.0)).astype(BF16)

    dg_start, dg_relay, dg_own, dg_finish = dg
    dg_start()
    gather_relay("early0", 1)
    square_rest(0, up_g)
    ig[0][0]()
    gather_relay("late", 2, (0,))
    ig[1][0]()
    dg_relay()
    gather_relay("late", 2, (1,))
    for d in range(3, last):
        gather_relay("late", d)
    for d in range(2, last):
        gather_own("early0", d)
        gather_own("early1", d)
    gather_relay("early1", 1)
    ig[0][1](1, True)
    gather_end("late")

    @pl.loop(0, side)
    def _(b):
        lt_s[b] = dot(late_g[...], up_g[b], 1, 0).astype(BF16)

    send(lt_s, lt_r, t_ss.at[1], t_rs.at[1], pn)
    ig[0][1](2, False)
    for d in range(2, last):
        gather_relay("early0", d)
    arrive(lt_r, t_ss.at[1], t_rs.at[1])

    @pl.loop(0, side)
    def _(b):
        pre = (lt_s[b].astype(F32) + lt_r[b].astype(F32)).astype(BF16)
        lp[b] = pre
        lh[b] = square_relu(pre)

    lo[0][0]()
    lo[1][0]()
    for o in range(1, a):
        zd = lax.rem(z + o, a)
        for u in range(half_side):
            b = mine(u)
            send(lp.at[b, slot(zd)], lp_g.at[:, columns(z * side + b, ff)],
                 l_ss.at[0, o, u], l_rs.at[0, o, u], (zd * side + q, t))
    ig[1][1](1, True)
    for d in range(2, last):
        gather_relay("early1", d)
    gather_end("early0")
    ug[0][0]()
    ig[1][1](2, False)
    ig[0][1](2, True)
    lo[0][1](1, True)
    dg_own()
    for copy in own_sums:
        copy.wait()
    dg_finish()
    ug[0][1]()
    ig[1][1](2, True)
    for k in range(3, last):
        for c in range(2):
            for opening in (False, True):
                ig[c][1](k, opening)
    gather_end("early1")
    ug[1][0]()
    lo[0][1](2, False)
    lo[0][1](2, True)
    lo[1][1](1, True)
    ug[1][1]()
    ig[0][2]()
    ig[1][2]()
    lo[1][1](2, False)
    lo[1][1](2, True)
    for k in range(3, last):
        for c in range(2):
            for opening in (False, True):
                lo[c][1](k, opening)
    for b in range(side):
        lp_g[:, columns(z * side + b, ff)] = lp[b, slot(z)]
    ug[0][2]()
    ug[1][2]()
    hops(mine, out_relay)
    ug[0][3]()
    lo[0][2]()
    ug[1][3]()
    lo[1][2]()
    hops(other, out_rest)
    late_pre_o[...] = lp_g[...]

    for cond, copy in sent:
        run(cond, copy.wait_send)


def store_body(*refs):
    n = len(refs) // 2
    sems = refs[2 * n]
    copies = [pltpu.make_async_copy(refs[k], refs[n + k], sems.at[k]) for k in range(n)]
    for copy in copies:
        copy.start()
    for copy in copies:
        copy.wait()


def store(results):
    n = len(results)
    return pl.pallas_call(
        store_body,
        out_shape=tuple(jax.ShapeDtypeStruct(r.shape, r.dtype) for r in results),
        in_specs=[pl.BlockSpec(memory_space=pltpu.VMEM)] * n,
        out_specs=[pl.BlockSpec(memory_space=pltpu.HBM)] * n,
        scratch_shapes=[pltpu.SemaphoreType.DMA((n,))],
        compiler_params=pltpu.CompilerParams(vmem_limit_bytes=16 * 1024 * 1024),
    )(*results)


def fused_body(late_input, up_weight, down_weight, early_input, early_pre, cotangent, up_sum, down_sum):
    a = lax.axis_size("fs") // 4
    side = 4
    rows, width = late_input.shape
    ff = up_weight.shape[1]
    tokens, hidden = rows * a, ff * side
    cut = width // 2
    V = pltpu.VMEM
    D = pltpu.SemaphoreType.DMA
    token_block = V((tokens, width), BF16)
    hidden_block = V((side, tokens, ff), BF16)
    line_block = V((2, a, rows, cut), BF16)
    scratch = (
        [token_block] * 2
        + [V((2, tokens, cut), BF16)]
        + [hidden_block, V((side, width, ff), BF16), V((side, ff, width), BF16)]
        + [hidden_block] * 8
        + [V((rows, hidden * a), BF16), V((2, 2, tokens, cut), F32)]
        + [line_block] * 6
        + [V((side, ff, width), BF16)] + [V((ff // 2, width), BF16)] * 2 + [V((ff, width), BF16)] * 2
        + [V((2, side, cut, ff), BF16)] + [V((2, cut // 2, ff), BF16)] * 2 + [V((2, cut, ff), BF16)] * 2
        + [D((6, 2, a)), D((6, 2, a)), D((2, 2, 3)), D((2, 2, 3)), D((2, a, 2)), D((2, a, 2)),
           D((2, a, 2)), D((2, a, 2)), D((2,)), D((2,)), D((2, 2, 2, a)), D((2, 2, 2, a)),
           D((2, 2, 6)), D((2, 2, 6)), D((13,))]
        + [V((width, ff), F32), V((ff, width), F32)]
    )
    flops = 12 * tokens * hidden * width
    results = pl.pallas_call(
        lambda *refs: fused(a, *refs),
        out_shape=(
            jax.ShapeDtypeStruct(early_pre.shape, BF16),
            jax.ShapeDtypeStruct(late_input.shape, BF16),
            jax.ShapeDtypeStruct(early_input.shape, BF16),
            jax.ShapeDtypeStruct(up_sum.shape, F32),
            jax.ShapeDtypeStruct(down_sum.shape, F32),
        ),
        in_specs=[pl.BlockSpec(memory_space=pltpu.HBM)] * 8,
        out_specs=[pl.BlockSpec(memory_space=pltpu.VMEM)] * 5,
        scratch_shapes=scratch,
        compiler_params=pltpu.CompilerParams(
            collective_id=0, has_side_effects=True, vmem_limit_bytes=48 * 1024 * 1024),
        cost_estimate=pl.CostEstimate(flops=flops, bytes_accessed=1 << 24, transcendentals=0),
    )(*[pltpu.with_memory_space_constraint(v, pltpu.HBM) for v in (
        late_input, up_weight, down_weight, early_input, early_pre, cotangent, up_sum, down_sum)])
    return store(results)


def contract_rows(left, right):
    return lax.dot_general(
        left, right, (((0,), (0,)), ((), ())), preferred_element_type=jnp.float32
    )


def contract_cols(left, right):
    return lax.dot_general(
        left, right, (((1,), (1,)), ((), ())), preferred_element_type=jnp.float32
    )


def body(late_input, up_weight, down_weight, early_input, early_pre, cotangent, up_sum, down_sum):
    up_gathered = lax.all_gather(up_weight, "fs", axis=1, tiled=True)
    down_gathered = lax.all_gather(down_weight, "fs", axis=0, tiled=True)
    pre_terms = jnp.dot(late_input, up_gathered, preferred_element_type=jnp.float32)
    pre_summed = lax.psum(pre_terms.astype(jnp.bfloat16), "tp")
    late_hidden = jnp.square(jax.nn.relu(pre_summed.astype(jnp.float32))).astype(jnp.bfloat16)
    early_float = early_pre.astype(jnp.float32)
    early_hidden = jnp.square(jax.nn.relu(early_float)).astype(jnp.bfloat16)
    late_out = jnp.dot(late_hidden, down_gathered, preferred_element_type=jnp.float32).astype(
        jnp.bfloat16
    )
    grad_terms = contract_cols(cotangent, down_gathered)
    hidden_grad = lax.psum(grad_terms.astype(jnp.bfloat16), "tp").astype(jnp.float32)
    pre_grad = (hidden_grad * 2.0 * jax.nn.relu(early_float)).astype(jnp.bfloat16)
    input_grad = contract_cols(pre_grad, up_gathered).astype(jnp.bfloat16)
    grad_local, hidden_local = (
        lax.all_to_all(pre_grad, "fs", split_axis=1, concat_axis=0, tiled=True),
        lax.all_to_all(early_hidden, "fs", split_axis=1, concat_axis=0, tiled=True),
    )
    rows = grad_local
    up_grad = contract_rows(lax.all_gather(early_input, "fs", axis=0, tiled=True), rows)
    up_total = up_sum + up_grad
    rows = hidden_local
    down_grad = contract_rows(rows, lax.all_gather(cotangent, "fs", axis=0, tiled=True))
    down_total = down_sum + down_grad
    return (pre_summed, late_out, input_grad, up_total, down_total)


def solution(mesh):
    in_specs = (
        P("fs", "tp"),
        P("tp", "fs"),
        P("fs", "tp"),
        P("fs", "tp"),
        P("fs", None),
        P("fs", "tp"),
        P("tp", "fs"),
        P("fs", "tp"),
    )
    out_specs = (P("fs", None), P("fs", "tp"), P("fs", "tp"), P("tp", "fs"), P("fs", "tp"))
    square_chips = mesh.shape["tp"] == 2 and mesh.shape["fs"] % 4 == 0 and mesh.shape["fs"] >= 8
    chosen = fused_body if square_chips else body
    return jax.shard_map(chosen, mesh=mesh, in_specs=in_specs, out_specs=out_specs, check_vma=False)
```

```python
from types import SimpleNamespace

import jax
import jax.numpy as jnp
from jax import lax
from jax.experimental import pallas as pl
from jax.experimental.pallas import tpu as pltpu
from jax.sharding import PartitionSpec as P

MESH = pl.DeviceIdType.MESH
F32 = jnp.float32
BF16 = jnp.bfloat16


def dot(left, right, lc, rc):
    return lax.dot_general(left, right, (((lc,), (rc,)), ((), ())), preferred_element_type=F32)


def square_relu(value):
    kept = jnp.maximum(value.astype(F32), 0.0)
    return (kept * kept).astype(BF16)


def fused(a, late_in, up_w, down_w, early_in, early_pre, cot, up_old, down_old,
          late_pre_o, lo_v, ig_v, up_v, down_v,
          cot_g, late_g, early_g, pre_g, up_g, down_g, gt_s, gt_r, pg, eh, lt_s, lt_r, lp, lh, lp_g,
          part, ig_s, ig_u, ig_d, lo_s, lo_u, lo_d,
          dg_s, dg_x, dg_y, dg_fx, dg_fy, ug_s, ug_x, ug_y, ug_fx, ug_fy,
          ag_ss, ag_rs, w_ss, w_rs, e_ss, e_rs, l_ss, l_rs, t_ss, t_rs, rl_ss, rl_rs, rq_ss, rq_rs,
          local_s, up_was, down_was):
    side = 4
    half_side = side // 2
    me = lax.axis_index("fs")
    t = lax.axis_index("tp")
    z = me // side
    q = lax.rem(me, side)
    y = q // 2
    x = lax.rem(q, 2)
    qx = y * 2 + (1 - x)
    qy = (1 - y) * 2 + x
    qd = side - 1 - q
    xn = (z * side + qx, t)
    yn = (z * side + qy, t)
    pn = (me, 1 - t)
    above = (lax.rem(me + side, a * side), t)
    below = (lax.rem(me + (a - 1) * side, a * side), t)
    rows = late_in.shape[0]
    ff = up_w.shape[1]
    width = late_in.shape[1]
    cut = width // 2
    last = a - 1
    middle = (z > 0) & (z < last)

    def begin(src, dst, k):
        copy = pltpu.make_async_copy(src, dst, local_s.at[k])
        copy.start()
        return copy

    def slot(j):
        return pl.ds(pl.multiple_of(j * rows, rows), rows)

    def slots(n):
        size = rows // n
        return lambda j, c: pl.ds(pl.multiple_of(j * rows + c * size, size), size)

    def columns(block, unit):
        return pl.ds(pl.multiple_of(block * unit, unit), unit)

    own_rows = slot(z)
    own_down = begin(down_w, down_g.at[q], 0)
    own_cot = begin(cot, cot_g.at[own_rows], 1)
    own_late = begin(late_in, late_g.at[own_rows], 3)
    own_early = [begin(early_in.at[:, pl.ds(c * cut, cut)], early_g.at[c, own_rows], 9 + c) for c in range(2)]
    own_up = begin(up_w, up_g.at[q], 2)
    own_pre = [
        begin(early_pre.at[:, pl.ds(pl.multiple_of((z * side + b) * ff, ff), ff)],
              pre_g.at[b, own_rows], 5 + b)
        for b in range(side)
    ]

    own_sums = [begin(up_old, up_was, 11), begin(down_old, down_was, 12)]

    barrier = pltpu.get_barrier_semaphore()
    greet = [xn, yn, pn] + [(lax.rem(me + o * side, a * side), t) for o in range(1, a)]
    for device in greet:
        pl.semaphore_signal(barrier, inc=1, device_id=device, device_id_type=MESH)
    pl.semaphore_wait(barrier, len(greet))

    sent = []

    def run(cond, go):
        if cond is None:
            go()
        else:
            pl.when(cond)(go)

    def rc(src, dst, ss, rs, device):
        return pltpu.make_async_remote_copy(
            src_ref=src, dst_ref=dst, send_sem=ss, recv_sem=rs, device_id=device, device_id_type=MESH)

    def send(src, dst, ss, rs, device, cond=None):
        copy = rc(src, dst, ss, rs, device)
        run(cond, copy.start)
        sent.append((cond, copy))

    def arrive(dst, ss, rs, cond=None):
        run(cond, rc(dst, dst, ss, rs, pn).wait_recv)

    gathers = {
        "cot": (0, 2, lambda j, c: cot_g.at[slots(2)(j, c)]),
        "late": (2, 2, lambda j, c: late_g.at[slots(2)(j, c)]),
        "early0": (4, 1, lambda j, c: early_g.at[0, slot(j)]),
        "early1": (5, 1, lambda j, c: early_g.at[1, slot(j)]),
    }

    def gather_own(name, depth=None):
        first, pieces, piece = gathers[name]
        for c in range(pieces):
            own = piece(z, c)
            for way, edge, device in ((0, z < last, above), (1, z > 0, below)):
                left = z if way == 0 else last - z
                cond = edge if depth is None else edge & (left == depth)
                send(own, own, ag_ss.at[first + c, way, 0], ag_rs.at[first + c, way, 1], device, cond)

    def gather_relay(name, d, some=None):
        if d >= last:
            return
        first, pieces, piece = gathers[name]
        for c in range(pieces) if some is None else some:
            for way, here, j, device in ((0, (z >= d) & (z < last), z - d, above),
                                         (1, (z + d < a) & (z > 0), z + d, below)):
                place = piece(jnp.clip(j, 0, last), c)
                arrive(place, ag_ss.at[first + c, way, 0], ag_rs.at[first + c, way, d], here)
                send(place, place, ag_ss.at[first + c, way, d], ag_rs.at[first + c, way, d + 1], device, here)

    def gather_end(name):
        first, pieces, piece = gathers[name]
        for d in range(1, a):
            for c in range(pieces):
                for way, here, j in ((0, z == last, z - d), (1, z == 0, z + d)):
                    place = piece(jnp.clip(j, 0, last), c)
                    arrive(place, ag_ss.at[first + c, way, 0], ag_rs.at[first + c, way, d], here)

    def half(ref, block, h):
        n = ref.shape[1] // 2
        return ref.at[block, pl.ds(h * n, n)]

    def half2(ref, h):
        n = ref.shape[0] // 2
        return ref.at[pl.ds(h * n, n)]

    def square_send(which, own, buf):
        for h in (0, 1):
            send(half2(own, h), half(buf, q, h), w_ss.at[which, 0, h], w_rs.at[which, 0, h], xn)
            send(half2(own, 1 - h), half(buf, q, 1 - h), w_ss.at[which, 1, 1 - h], w_rs.at[which, 1, 1 - h], yn)

    def square_relay(which, buf):
        arrive(half(buf, qx, 0), w_ss.at[which, 0, 0], w_rs.at[which, 0, 0])
        send(half(buf, qx, 0), half(buf, qx, 0), w_ss.at[which, 1, 2], w_rs.at[which, 1, 2], yn)
        arrive(half(buf, qy, 1), w_ss.at[which, 0, 0], w_rs.at[which, 1, 1])
        send(half(buf, qy, 1), half(buf, qy, 1), w_ss.at[which, 0, 2], w_rs.at[which, 0, 2], xn)

    def square_rest(which, buf):
        arrive(half(buf, qx, 1), w_ss.at[which, 0, 0], w_rs.at[which, 0, 1])
        arrive(half(buf, qy, 0), w_ss.at[which, 0, 0], w_rs.at[which, 1, 0])
        arrive(half(buf, qd, 0), w_ss.at[which, 0, 0], w_rs.at[which, 1, 2])
        arrive(half(buf, qd, 1), w_ss.at[which, 0, 0], w_rs.at[which, 0, 2])

    def square_sum(which, c, block, staged, first_x, first_y, fin_x, fin_y, was, out):
        n = staged.shape[1] // 2
        sems = lambda k: (rq_ss.at[which, c, k], rq_rs.at[which, c, k])
        wait = lambda dst, k: arrive(dst, *sems(k))

        def start():
            staged[qd] = block(qd).astype(BF16)
            send(half(staged, qd, 0), first_x, *sems(0), xn)
            send(half(staged, qd, 1), first_y, *sems(1), yn)
            staged[qx] = block(qx).astype(BF16)
            send(half(staged, qx, 0), half2(fin_x, 0), *sems(2), xn)
            staged[qy] = block(qy).astype(BF16)
            send(half(staged, qy, 1), half2(fin_y, 1), *sems(3), yn)

        def relay():
            wait(first_x, 0)
            staged[qy, 0:n] = (staged[qy, 0:n].astype(F32) + first_x[...].astype(F32)).astype(BF16)
            send(half(staged, qy, 0), half2(fin_y, 0), *sems(4), yn)
            wait(first_y, 1)
            staged[qx, n:2 * n] = (staged[qx, n:2 * n].astype(F32) + first_y[...].astype(F32)).astype(BF16)
            send(half(staged, qx, 1), half2(fin_x, 1), *sems(5), xn)

        def own():
            out[...] = block(q)

        def finish():
            wait(half2(fin_x, 0), 2)
            wait(half2(fin_y, 1), 3)
            wait(half2(fin_y, 0), 4)
            wait(half2(fin_x, 1), 5)
            out[...] = was[...] + (out[...] + (fin_x[...].astype(F32) + fin_y[...].astype(F32)))

        return SimpleNamespace(start=start, relay=relay, own=own, finish=finish)

    def line_sum(which, c, value, staged, from_u, from_d, out):
        own = part.at[which, c]

        def go(way, j, step, cond):
            buf, device = ((from_u, above), (from_d, below))[way]
            send(staged.at[c, j], buf.at[c, j], rl_ss.at[which, c, way, step], rl_rs.at[which, c, way, j], device, cond)

        def start():
            own[...] = value(c)
            for j in range(a):
                staged[c, j] = own[pl.ds(j * rows, rows)].astype(BF16)
            for step in range(last):
                go(0, last - step, step, z == 0)
                go(1, step, step, z == last)

        def relay(step, opening):
            if step >= last:
                return
            for way in range(2):
                if way == 0:
                    j, on, opens, buf = last + z - step, step >= z, z == step, from_u
                else:
                    j, on, opens, buf = step - (last - z), step >= last - z, last - z == step, from_d
                on = on & middle & (opens if opening else jnp.logical_not(opens))
                j = jnp.clip(j, 0, last)

                @pl.when(on)
                def _(j=j, buf=buf, way=way):
                    arrive(buf.at[c, j], rl_ss.at[which, 0, 0, 0], rl_rs.at[which, c, way, j])
                    staged[c, j] = (staged[c, j].astype(F32) + buf[c, j].astype(F32)).astype(BF16)

                go(way, j, step, on)

        def finish():
            @pl.when(z > 0)
            def _():
                arrive(from_u.at[c, z], rl_ss.at[which, 0, 0, 0], rl_rs.at[which, c, 0, z])
                own[own_rows] = own[own_rows] + from_u[c, z].astype(F32)

            @pl.when(z < last)
            def _():
                arrive(from_d.at[c, z], rl_ss.at[which, 0, 0, 0], rl_rs.at[which, c, 1, z])
                own[own_rows] = own[own_rows] + from_d[c, z].astype(F32)

            out[:, pl.ds(c * cut, cut)] = own[own_rows].astype(BF16)

        return SimpleNamespace(start=start, relay=relay, finish=finish)

    def hops(b_of, go, offsets=None):
        for o in range(1, a) if offsets is None else offsets:
            if o < a:
                zs = lax.rem(z - o + a, a)
                for u in range(half_side):
                    go(o, u, zs, b_of(u))

    mine = lambda u: t * half_side + u
    other = lambda u: (1 - t) * half_side + u

    def spread(source, target, ss, rs):
        for k in range(last, 0, -1):
            for o, cond in ((k, z + k <= last), (a - k, z >= k)):
                zd = lax.rem(z + o, a)
                for u in range(half_side):
                    b = mine(u)
                    send(source(zd, b), target(b), ss.at[0, o, u], rs.at[0, o, u], (zd * side + q, t), cond)

    def pre_relay(o, u, zs, b):
        place = pre_g.at[b, slot(zs)]
        arrive(place, e_ss.at[0, 0, 0], e_rs.at[0, o, u])
        send(place, place, e_ss.at[1, o, u], e_rs.at[1, o, u], pn)

    def pre_rest(o, u, zs, b):
        arrive(pre_g.at[b, slot(zs)], e_ss.at[0, 0, 0], e_rs.at[1, o, u])

    def out_relay(o, u, zs, b):
        place = lp_g.at[:, columns(zs * side + b, ff)]
        arrive(place, l_ss.at[0, 0, 0], l_rs.at[0, o, u])
        send(place, place, l_ss.at[1, o, u], l_rs.at[1, o, u], pn)
        late_pre_o[:, columns(zs * side + b, ff)] = place[...]

    def out_rest(o, u, zs, b):
        place = lp_g.at[:, columns(zs * side + b, ff)]
        arrive(place, l_ss.at[0, 0, 0], l_rs.at[1, o, u])
        late_pre_o[:, columns(zs * side + b, ff)] = place[...]

    def ig_value(c):
        return sum(dot(pg[b], up_g[b, pl.ds(c * cut, cut), :], 1, 1) for b in range(side))

    def lo_value(c):
        return sum(dot(lh[b], down_g[b, :, pl.ds(c * cut, cut)], 1, 0) for b in range(side))

    ig = [line_sum(0, c, ig_value, ig_s, ig_u, ig_d, ig_v) for c in range(2)]
    lo = [line_sum(1, c, lo_value, lo_s, lo_u, lo_d, lo_v) for c in range(2)]
    dg = square_sum(1, 0, lambda b: dot(eh[b], cot_g[...], 0, 0), dg_s, dg_x, dg_y, dg_fx, dg_fy, down_was, down_v)
    ug = [
        square_sum(0, c, lambda b, c=c: dot(early_g[c], pg[b], 0, 0), ug_s.at[c], ug_x.at[c], ug_y.at[c],
                   ug_fx.at[c], ug_fy.at[c], up_was.at[pl.ds(c * cut, cut)], up_v.at[pl.ds(c * cut, cut)])
        for c in range(2)
    ]

    def hidden_grad_terms():
        gather_end("cot")
        square_rest(1, down_g)

        @pl.loop(0, side)
        def _(b):
            gt_s[b] = dot(cot_g[...], down_g[b], 1, 1).astype(BF16)

        send(gt_s, gt_r, t_ss.at[0], t_rs.at[0], pn)

    def early_hidden():
        for copy in own_pre + own_sums:
            copy.wait()
        hops(other, pre_rest)

        @pl.loop(0, side)
        def _(b):
            eh[b] = square_relu(pre_g[b])

    def pre_grad():
        arrive(gt_r, t_ss.at[0], t_rs.at[0])

        @pl.loop(0, side)
        def _(b):
            hidden = gt_s[b].astype(F32) + gt_r[b].astype(F32)
            pg[b] = (hidden * 2.0 * jnp.maximum(pre_g[b].astype(F32), 0.0)).astype(BF16)

    def late_terms():
        gather_end("late")

        @pl.loop(0, side)
        def _(b):
            lt_s[b] = dot(late_g[...], up_g[b], 1, 0).astype(BF16)

        send(lt_s, lt_r, t_ss.at[1], t_rs.at[1], pn)

    def late_hidden():
        arrive(lt_r, t_ss.at[1], t_rs.at[1])

        @pl.loop(0, side)
        def _(b):
            pre = (lt_s[b].astype(F32) + lt_r[b].astype(F32)).astype(BF16)
            lp[b] = pre
            lh[b] = square_relu(pre)

    def send_pre():
        spread(lambda zd, b: early_pre.at[:, columns(zd * side + b, ff)],
               lambda b: pre_g.at[b, slot(z)], e_ss, e_rs)

    def send_late_pre():
        spread(lambda zd, b: lp.at[b, slot(zd)],
               lambda b: lp_g.at[:, columns(z * side + b, ff)], l_ss, l_rs)

    def keep_own():
        ug[0].own()
        ug[1].own()
        for b in range(side):
            late_pre_o[:, columns(z * side + b, ff)] = lp[b, slot(z)]

    def down_finish():
        dg.own()
        dg.finish()

    def relay_rest(name, some=None):
        for d in range(2, last):
            gather_relay(name, d, some)

    def own_rest(name):
        for d in range(2, last):
            gather_own(name, d)

    def line_rest(chain):
        chain.relay(2, True)
        for k in range(3, last):
            chain.relay(k, False)
            chain.relay(k, True)

    own_down.wait()
    square_send(1, down_g.at[q], down_g)
    own_cot.wait()
    gather_own("cot")
    gather_relay("cot", 1)
    square_relay(1, down_g)
    send_pre()
    own_late.wait()
    gather_own("late", 1)
    relay_rest("cot")
    own_early[0].wait()
    gather_own("early0", 1)
    gather_own("late", 0)
    own_up.wait()
    square_send(0, up_g.at[q], up_g)
    hops(mine, pre_relay, range(3, a))
    own_rest("late")
    square_relay(0, up_g)
    hops(mine, pre_relay, (1,))
    gather_own("early0", 0)
    gather_relay("late", 1, (0,))
    gather_relay("late", 1, (1,))
    hops(mine, pre_relay, (2,))
    hidden_grad_terms()
    own_early[1].wait()
    gather_own("early1", 0)
    gather_own("early1", 1)
    early_hidden()
    pre_grad()
    gather_relay("early0", 1)
    dg.start()
    relay_rest("late", (0,))
    relay_rest("late", (1,))
    square_rest(0, up_g)
    ig[0].start()
    gather_relay("early1", 1)
    own_rest("early0")
    ig[1].start()
    ig[0].relay(1, True)
    own_rest("early1")
    relay_rest("early0")
    late_terms()
    ig[0].relay(2, False)
    late_hidden()
    ig[1].relay(1, True)
    relay_rest("early1")
    lo[0].start()
    dg.relay()
    lo[1].start()
    ig[1].relay(2, False)
    gather_end("early0")
    ug[0].start()
    gather_end("early1")
    ug[1].start()
    send_late_pre()
    line_rest(ig[0])
    lo[0].relay(1, True)
    keep_own()
    lo[1].relay(1, True)
    line_rest(ig[1])
    lo[0].relay(2, False)
    ug[0].relay()
    ig[1].finish()
    ug[1].relay()
    line_rest(lo[0])
    ug[0].finish()
    ig[0].finish()
    lo[1].relay(2, False)
    line_rest(lo[1])
    down_finish()
    lo[0].finish()
    hops(mine, out_relay, (2,))
    hops(mine, out_relay, range(3, a))
    hops(mine, out_relay, (1,))
    ug[1].finish()
    lo[1].finish()
    hops(other, out_rest)

    for cond, copy in sent:
        run(cond, copy.wait_send)


def store_body(*refs):
    n = len(refs) // 2
    sems = refs[2 * n]
    copies = [pltpu.make_async_copy(refs[k], refs[n + k], sems.at[k]) for k in range(n)]
    for copy in copies:
        copy.start()
    for copy in copies:
        copy.wait()


def store(results):
    n = len(results)
    return pl.pallas_call(
        store_body,
        out_shape=tuple(jax.ShapeDtypeStruct(r.shape, r.dtype) for r in results),
        in_specs=[pl.BlockSpec(memory_space=pltpu.VMEM)] * n,
        out_specs=[pl.BlockSpec(memory_space=pltpu.HBM)] * n,
        scratch_shapes=[pltpu.SemaphoreType.DMA((n,))],
        compiler_params=pltpu.CompilerParams(vmem_limit_bytes=16 * 1024 * 1024),
    )(*results)


def fused_body(late_input, up_weight, down_weight, early_input, early_pre, cotangent, up_sum, down_sum):
    a = lax.axis_size("fs") // 4
    side = 4
    rows, width = late_input.shape
    ff = up_weight.shape[1]
    tokens, hidden = rows * a, ff * side
    cut = width // 2
    V = pltpu.VMEM
    D = pltpu.SemaphoreType.DMA
    token_block = V((tokens, width), BF16)
    hidden_block = V((side, tokens, ff), BF16)
    line_block = V((2, a, rows, cut), BF16)
    scratch = (
        [token_block] * 2
        + [V((2, tokens, cut), BF16)]
        + [hidden_block, V((side, width, ff), BF16), V((side, ff, width), BF16)]
        + [hidden_block] * 8
        + [V((rows, hidden * a), BF16), V((2, 2, tokens, cut), F32)]
        + [line_block] * 6
        + [V((side, ff, width), BF16)] + [V((ff // 2, width), BF16)] * 2 + [V((ff, width), BF16)] * 2
        + [V((2, side, cut, ff), BF16)] + [V((2, cut // 2, ff), BF16)] * 2 + [V((2, cut, ff), BF16)] * 2
        + [D((6, 2, a)), D((6, 2, a)), D((2, 2, 3)), D((2, 2, 3)), D((2, a, 2)), D((2, a, 2)),
           D((2, a, 2)), D((2, a, 2)), D((2,)), D((2,)), D((2, 2, 2, a)), D((2, 2, 2, a)),
           D((2, 2, 6)), D((2, 2, 6)), D((13,))]
        + [V((width, ff), F32), V((ff, width), F32)]
    )
    flops = 12 * tokens * hidden * width
    results = pl.pallas_call(
        lambda *refs: fused(a, *refs),
        out_shape=(
            jax.ShapeDtypeStruct(early_pre.shape, BF16),
            jax.ShapeDtypeStruct(late_input.shape, BF16),
            jax.ShapeDtypeStruct(early_input.shape, BF16),
            jax.ShapeDtypeStruct(up_sum.shape, F32),
            jax.ShapeDtypeStruct(down_sum.shape, F32),
        ),
        in_specs=[pl.BlockSpec(memory_space=pltpu.HBM)] * 8,
        out_specs=[pl.BlockSpec(memory_space=pltpu.VMEM)] * 5,
        scratch_shapes=scratch,
        compiler_params=pltpu.CompilerParams(
            collective_id=0, has_side_effects=True, vmem_limit_bytes=48 * 1024 * 1024),
        cost_estimate=pl.CostEstimate(flops=flops, bytes_accessed=1 << 24, transcendentals=0),
    )(*[pltpu.with_memory_space_constraint(v, pltpu.HBM) for v in (
        late_input, up_weight, down_weight, early_input, early_pre, cotangent, up_sum, down_sum)])
    return store(results)


def contract_rows(left, right):
    return lax.dot_general(
        left, right, (((0,), (0,)), ((), ())), preferred_element_type=jnp.float32
    )


def contract_cols(left, right):
    return lax.dot_general(
        left, right, (((1,), (1,)), ((), ())), preferred_element_type=jnp.float32
    )


def body(late_input, up_weight, down_weight, early_input, early_pre, cotangent, up_sum, down_sum):
    up_gathered = lax.all_gather(up_weight, "fs", axis=1, tiled=True)
    down_gathered = lax.all_gather(down_weight, "fs", axis=0, tiled=True)
    pre_terms = jnp.dot(late_input, up_gathered, preferred_element_type=jnp.float32)
    pre_summed = lax.psum(pre_terms.astype(jnp.bfloat16), "tp")
    late_hidden = jnp.square(jax.nn.relu(pre_summed.astype(jnp.float32))).astype(jnp.bfloat16)
    early_float = early_pre.astype(jnp.float32)
    early_hidden = jnp.square(jax.nn.relu(early_float)).astype(jnp.bfloat16)
    late_out = jnp.dot(late_hidden, down_gathered, preferred_element_type=jnp.float32).astype(
        jnp.bfloat16
    )
    grad_terms = contract_cols(cotangent, down_gathered)
    hidden_grad = lax.psum(grad_terms.astype(jnp.bfloat16), "tp").astype(jnp.float32)
    pre_grad = (hidden_grad * 2.0 * jax.nn.relu(early_float)).astype(jnp.bfloat16)
    input_grad = contract_cols(pre_grad, up_gathered).astype(jnp.bfloat16)
    grad_local, hidden_local = (
        lax.all_to_all(pre_grad, "fs", split_axis=1, concat_axis=0, tiled=True),
        lax.all_to_all(early_hidden, "fs", split_axis=1, concat_axis=0, tiled=True),
    )
    rows = grad_local
    up_grad = contract_rows(lax.all_gather(early_input, "fs", axis=0, tiled=True), rows)
    up_total = up_sum + up_grad
    rows = hidden_local
    down_grad = contract_rows(rows, lax.all_gather(cotangent, "fs", axis=0, tiled=True))
    down_total = down_sum + down_grad
    return (pre_summed, late_out, input_grad, up_total, down_total)


def solution(mesh):
    in_specs = (
        P("fs", "tp"),
        P("tp", "fs"),
        P("fs", "tp"),
        P("fs", "tp"),
        P("fs", None),
        P("fs", "tp"),
        P("tp", "fs"),
        P("fs", "tp"),
    )
    out_specs = (P("fs", None), P("fs", "tp"), P("fs", "tp"), P("tp", "fs"), P("fs", "tp"))
    square_chips = mesh.shape["tp"] == 2 and mesh.shape["fs"] % 4 == 0 and mesh.shape["fs"] >= 8
    chosen = fused_body if square_chips else body
    return jax.shard_map(chosen, mesh=mesh, in_specs=in_specs, out_specs=out_specs, check_vma=False)
```

```python
from types import SimpleNamespace

import jax
import jax.numpy as jnp
from jax import lax
from jax.experimental import pallas as pl
from jax.experimental.pallas import tpu as pltpu
from jax.sharding import PartitionSpec as P

MESH = pl.DeviceIdType.MESH
F32 = jnp.float32
BF16 = jnp.bfloat16


def dot(left, right, lc, rc):
    return lax.dot_general(left, right, (((lc,), (rc,)), ((), ())), preferred_element_type=F32)


def square_relu(value):
    kept = jnp.maximum(value.astype(F32), 0.0)
    return (kept * kept).astype(BF16)


def fused(a, late_in, up_w, down_w, early_in, early_pre, cot, up_old, down_old,
          late_pre_o, lo_v, ig_v, up_v, down_v,
          cot_g, late_g, early_g, pre_g, up_g, down_g, gt_s, gt_r, pg, eh, lt_s, lt_r, lp, lh, lp_g,
          part, ig_s, ig_u, ig_d, lo_s, lo_u, lo_d,
          dg_s, dg_x, dg_y, dg_fx, dg_fy, ug_s, ug_x, ug_y, ug_fx, ug_fy,
          ag_ss, ag_rs, w_ss, w_rs, e_ss, e_rs, l_ss, l_rs, t_ss, t_rs, rl_ss, rl_rs, rq_ss, rq_rs,
          local_s, up_was, down_was, line_s):
    side = 4
    half_side = side // 2
    me = lax.axis_index("fs")
    t = lax.axis_index("tp")
    z = me // side
    q = lax.rem(me, side)
    y = q // 2
    x = lax.rem(q, 2)
    qx = y * 2 + (1 - x)
    qy = (1 - y) * 2 + x
    qd = side - 1 - q
    xn = (z * side + qx, t)
    yn = (z * side + qy, t)
    pn = (me, 1 - t)
    above = (lax.rem(me + side, a * side), t)
    below = (lax.rem(me + (a - 1) * side, a * side), t)
    rows = late_in.shape[0]
    ff = up_w.shape[1]
    width = late_in.shape[1]
    cut = width // 2
    last = a - 1
    middle = (z > 0) & (z < last)

    def begin(src, dst, k):
        copy = pltpu.make_async_copy(src, dst, local_s.at[k])
        copy.start()
        return copy

    def slot(j):
        return pl.ds(pl.multiple_of(j * rows, rows), rows)

    def slots(n):
        size = rows // n
        return lambda j, c: pl.ds(pl.multiple_of(j * rows + c * size, size), size)

    def columns(block, unit):
        return pl.ds(pl.multiple_of(block * unit, unit), unit)

    own_rows = slot(z)
    own_cot = begin(cot, cot_g.at[own_rows], 1)
    own_down = begin(down_w, down_g.at[q], 0)
    own_late = begin(late_in, late_g.at[own_rows], 3)
    own_early = [begin(early_in.at[:, pl.ds(c * cut, cut)], early_g.at[c, own_rows], 9 + c) for c in range(2)]
    own_up = begin(up_w, up_g.at[q], 2)
    own_pre = [
        begin(early_pre.at[:, pl.ds(pl.multiple_of((z * side + b) * ff, ff), ff)],
              pre_g.at[b, own_rows], 5 + b)
        for b in range(side)
    ]


    barrier = pltpu.get_barrier_semaphore()
    has_above = z < last
    has_below = z > 0

    def signal(semaphore, device):
        pl.semaphore_signal(semaphore, inc=1, device_id=device, device_id_type=MESH)

    for device in (xn, yn, pn):
        signal(barrier, device)
    pl.when(has_above)(lambda: signal(barrier, above))
    pl.when(has_below)(lambda: signal(barrier, below))
    pl.semaphore_wait(barrier, 3 + jnp.where(has_above, 1, 0) + jnp.where(has_below, 1, 0))

    def line_entered():
        pl.when(has_above)(lambda: pl.semaphore_wait(line_s.at[0], 1))
        pl.when(has_below)(lambda: signal(line_s.at[0], below))
        pl.when(has_below)(lambda: pl.semaphore_wait(line_s.at[1], 1))
        pl.when(has_above)(lambda: signal(line_s.at[1], above))

    sent = []

    def run(cond, go):
        if cond is None:
            go()
        else:
            pl.when(cond)(go)

    def rc(src, dst, ss, rs, device):
        return pltpu.make_async_remote_copy(
            src_ref=src, dst_ref=dst, send_sem=ss, recv_sem=rs, device_id=device, device_id_type=MESH)

    def send(src, dst, ss, rs, device, cond=None):
        copy = rc(src, dst, ss, rs, device)
        run(cond, copy.start)
        sent.append((cond, copy))

    def settle(count):
        for cond, copy in sent[:count]:
            run(cond, copy.wait_send)
        del sent[:count]

    def arrive(dst, ss, rs, cond=None):
        run(cond, rc(dst, dst, ss, rs, pn).wait_recv)

    gathers = {
        "cot": (0, 2, lambda j, c: cot_g.at[slots(2)(j, c)]),
        "late": (2, 2, lambda j, c: late_g.at[slots(2)(j, c)]),
        "early0": (4, 1, lambda j, c: early_g.at[0, slot(j)]),
        "early1": (5, 1, lambda j, c: early_g.at[1, slot(j)]),
    }

    def gather_own(name, depth=None):
        first, pieces, piece = gathers[name]
        for c in range(pieces):
            own = piece(z, c)
            for way, edge, device in ((0, z < last, above), (1, z > 0, below)):
                left = z if way == 0 else last - z
                cond = edge if depth is None else edge & (left == depth)
                send(own, own, ag_ss.at[first + c, way, 0], ag_rs.at[first + c, way, 1], device, cond)

    def gather_relay(name, d, some=None):
        if d >= last:
            return
        first, pieces, piece = gathers[name]
        for c in range(pieces) if some is None else some:
            for way, here, j, device in ((0, (z >= d) & (z < last), z - d, above),
                                         (1, (z + d < a) & (z > 0), z + d, below)):
                place = piece(jnp.clip(j, 0, last), c)
                arrive(place, ag_ss.at[first + c, way, 0], ag_rs.at[first + c, way, d], here)
                send(place, place, ag_ss.at[first + c, way, d], ag_rs.at[first + c, way, d + 1], device, here)

    def gather_end(name):
        first, pieces, piece = gathers[name]
        for d in range(1, a):
            for c in range(pieces):
                for way, here, j in ((0, z == last, z - d), (1, z == 0, z + d)):
                    place = piece(jnp.clip(j, 0, last), c)
                    arrive(place, ag_ss.at[first + c, way, 0], ag_rs.at[first + c, way, d], here)

    def half(ref, block, h):
        n = ref.shape[1] // 2
        return ref.at[block, pl.ds(h * n, n)]

    def half2(ref, h):
        n = ref.shape[0] // 2
        return ref.at[pl.ds(h * n, n)]

    def square_send(which, own, buf):
        for h in (0, 1):
            send(half2(own, h), half(buf, q, h), w_ss.at[which, 0, h], w_rs.at[which, 0, h], xn)
            send(half2(own, 1 - h), half(buf, q, 1 - h), w_ss.at[which, 1, 1 - h], w_rs.at[which, 1, 1 - h], yn)

    def square_relay(which, buf):
        arrive(half(buf, qx, 0), w_ss.at[which, 0, 0], w_rs.at[which, 0, 0])
        send(half(buf, qx, 0), half(buf, qx, 0), w_ss.at[which, 1, 2], w_rs.at[which, 1, 2], yn)
        arrive(half(buf, qy, 1), w_ss.at[which, 0, 0], w_rs.at[which, 1, 1])
        send(half(buf, qy, 1), half(buf, qy, 1), w_ss.at[which, 0, 2], w_rs.at[which, 0, 2], xn)

    def square_rest(which, buf):
        arrive(half(buf, qx, 1), w_ss.at[which, 0, 0], w_rs.at[which, 0, 1])
        arrive(half(buf, qy, 0), w_ss.at[which, 0, 0], w_rs.at[which, 1, 0])
        arrive(half(buf, qd, 0), w_ss.at[which, 0, 0], w_rs.at[which, 1, 2])
        arrive(half(buf, qd, 1), w_ss.at[which, 0, 0], w_rs.at[which, 0, 2])

    def square_sum(which, c, block, staged, first_x, first_y, fin_x, fin_y, was, out):
        n = staged.shape[1] // 2
        sems = lambda k: (rq_ss.at[which, c, k], rq_rs.at[which, c, k])
        wait = lambda dst, k: arrive(dst, *sems(k))

        def start():
            staged[qd] = block(qd).astype(BF16)
            send(half(staged, qd, 0), first_x, *sems(0), xn)
            send(half(staged, qd, 1), first_y, *sems(1), yn)
            staged[qx] = block(qx).astype(BF16)
            send(half(staged, qx, 0), half2(fin_x, 0), *sems(2), xn)
            staged[qy] = block(qy).astype(BF16)
            send(half(staged, qy, 1), half2(fin_y, 1), *sems(3), yn)

        def relay():
            wait(first_x, 0)
            staged[qy, 0:n] = (staged[qy, 0:n].astype(F32) + first_x[...].astype(F32)).astype(BF16)
            send(half(staged, qy, 0), half2(fin_y, 0), *sems(4), yn)
            wait(first_y, 1)
            staged[qx, n:2 * n] = (staged[qx, n:2 * n].astype(F32) + first_y[...].astype(F32)).astype(BF16)
            send(half(staged, qx, 1), half2(fin_x, 1), *sems(5), xn)

        def own():
            out[...] = block(q)

        def finish():
            wait(half2(fin_x, 0), 2)
            wait(half2(fin_y, 1), 3)
            wait(half2(fin_y, 0), 4)
            wait(half2(fin_x, 1), 5)
            out[...] = was[...] + (out[...] + (fin_x[...].astype(F32) + fin_y[...].astype(F32)))

        return SimpleNamespace(start=start, relay=relay, own=own, finish=finish)

    def line_sum(which, c, value, staged, from_u, from_d, out):
        own = part.at[which, c]

        def go(way, j, step, cond):
            buf, device = ((from_u, above), (from_d, below))[way]
            send(staged.at[c, j], buf.at[c, j], rl_ss.at[which, c, way, step], rl_rs.at[which, c, way, j], device, cond)

        def start():
            own[...] = value(c)
            for j in range(a):
                staged[c, j] = own[pl.ds(j * rows, rows)].astype(BF16)
            for step in range(last):
                go(0, last - step, step, z == 0)
                go(1, step, step, z == last)

        def relay(step, opening):
            if step >= last:
                return
            for way in range(2):
                if way == 0:
                    j, on, opens, buf = last + z - step, step >= z, z == step, from_u
                else:
                    j, on, opens, buf = step - (last - z), step >= last - z, last - z == step, from_d
                on = on & middle & (opens if opening else jnp.logical_not(opens))
                j = jnp.clip(j, 0, last)

                @pl.when(on)
                def _(j=j, buf=buf, way=way):
                    arrive(buf.at[c, j], rl_ss.at[which, 0, 0, 0], rl_rs.at[which, c, way, j])
                    staged[c, j] = (staged[c, j].astype(F32) + buf[c, j].astype(F32)).astype(BF16)

                go(way, j, step, on)

        def finish():
            @pl.when(z > 0)
            def _():
                arrive(from_u.at[c, z], rl_ss.at[which, 0, 0, 0], rl_rs.at[which, c, 0, z])
                own[own_rows] = own[own_rows] + from_u[c, z].astype(F32)

            @pl.when(z < last)
            def _():
                arrive(from_d.at[c, z], rl_ss.at[which, 0, 0, 0], rl_rs.at[which, c, 1, z])
                own[own_rows] = own[own_rows] + from_d[c, z].astype(F32)

            out[:, pl.ds(c * cut, cut)] = own[own_rows].astype(BF16)

        return SimpleNamespace(start=start, relay=relay, finish=finish)

    def hops(b_of, go, offsets=None):
        for o in range(1, a) if offsets is None else offsets:
            if o < a:
                zs = lax.rem(z - o + a, a)
                for u in range(half_side):
                    go(o, u, zs, b_of(u))

    mine = lambda u: t * half_side + u
    other = lambda u: (1 - t) * half_side + u

    def spread(source, target, ss, rs):
        for k in range(last, 0, -1):
            for o, cond in ((k, z + k <= last), (a - k, z >= k)):
                zd = lax.rem(z + o, a)
                for u in range(half_side):
                    b = mine(u)
                    send(source(zd, b), target(b), ss.at[0, o, u], rs.at[0, o, u], (zd * side + q, t), cond)

    def pre_relay(o, u, zs, b):
        place = pre_g.at[b, slot(zs)]
        arrive(place, e_ss.at[0, 0, 0], e_rs.at[0, o, u])
        send(place, place, e_ss.at[1, o, u], e_rs.at[1, o, u], pn)

    def pre_rest(o, u, zs, b):
        arrive(pre_g.at[b, slot(zs)], e_ss.at[0, 0, 0], e_rs.at[1, o, u])

    def out_relay(o, u, zs, b):
        place = lp_g.at[:, columns(zs * side + b, ff)]
        arrive(place, l_ss.at[0, 0, 0], l_rs.at[0, o, u])
        send(place, place, l_ss.at[1, o, u], l_rs.at[1, o, u], pn)
        late_pre_o[:, columns(zs * side + b, ff)] = place[...]

    def out_rest(o, u, zs, b):
        place = lp_g.at[:, columns(zs * side + b, ff)]
        arrive(place, l_ss.at[0, 0, 0], l_rs.at[1, o, u])
        late_pre_o[:, columns(zs * side + b, ff)] = place[...]

    def ig_value(c):
        return sum(dot(pg[b], up_g[b, pl.ds(c * cut, cut), :], 1, 1) for b in range(side))

    def lo_value(c):
        return sum(dot(lh[b], down_g[b, :, pl.ds(c * cut, cut)], 1, 0) for b in range(side))

    ig = [line_sum(0, c, ig_value, ig_s, ig_u, ig_d, ig_v) for c in range(2)]
    lo = [line_sum(1, c, lo_value, lo_s, lo_u, lo_d, lo_v) for c in range(2)]
    dg = square_sum(1, 0, lambda b: dot(eh[b], cot_g[...], 0, 0), dg_s, dg_x, dg_y, dg_fx, dg_fy, down_was, down_v)
    ug = [
        square_sum(0, c, lambda b, c=c: dot(early_g[c], pg[b], 0, 0), ug_s.at[c], ug_x.at[c], ug_y.at[c],
                   ug_fx.at[c], ug_fy.at[c], up_was.at[pl.ds(c * cut, cut)], up_v.at[pl.ds(c * cut, cut)])
        for c in range(2)
    ]

    def hidden_grad_terms():
        gather_end("cot")
        square_rest(1, down_g)

        @pl.loop(0, side)
        def _(b):
            gt_s[b] = dot(cot_g[...], down_g[b], 1, 1).astype(BF16)

        send(gt_s, gt_r, t_ss.at[0], t_rs.at[0], pn)

    def early_hidden():
        for copy in own_pre + own_sums:
            copy.wait()
        hops(other, pre_rest)

        @pl.loop(0, side)
        def _(b):
            eh[b] = square_relu(pre_g[b])

    def pre_grad():
        arrive(gt_r, t_ss.at[0], t_rs.at[0])

        @pl.loop(0, side)
        def _(b):
            hidden = gt_s[b].astype(F32) + gt_r[b].astype(F32)
            pg[b] = (hidden * 2.0 * jnp.maximum(pre_g[b].astype(F32), 0.0)).astype(BF16)

    def late_terms():
        gather_end("late")

        @pl.loop(0, side)
        def _(b):
            lt_s[b] = dot(late_g[...], up_g[b], 1, 0).astype(BF16)

        send(lt_s, lt_r, t_ss.at[1], t_rs.at[1], pn)

    def late_hidden():
        arrive(lt_r, t_ss.at[1], t_rs.at[1])

        @pl.loop(0, side)
        def _(b):
            pre = (lt_s[b].astype(F32) + lt_r[b].astype(F32)).astype(BF16)
            lp[b] = pre
            lh[b] = square_relu(pre)

    def send_pre():
        spread(lambda zd, b: early_pre.at[:, columns(zd * side + b, ff)],
               lambda b: pre_g.at[b, slot(z)], e_ss, e_rs)

    def send_late_pre():
        spread(lambda zd, b: lp.at[b, slot(zd)],
               lambda b: lp_g.at[:, columns(z * side + b, ff)], l_ss, l_rs)

    def keep_own():
        ug[0].own()
        ug[1].own()
        for b in range(side):
            late_pre_o[:, columns(z * side + b, ff)] = lp[b, slot(z)]

    def down_finish():
        dg.own()
        dg.finish()

    def relay_rest(name, some=None):
        for d in range(2, last):
            gather_relay(name, d, some)

    def own_rest(name):
        for d in range(2, last):
            gather_own(name, d)

    def line_rest(chain):
        chain.relay(2, True)
        for k in range(3, last):
            chain.relay(k, False)
            chain.relay(k, True)

    own_cot.wait()
    gather_own("cot")
    own_down.wait()
    square_send(1, down_g.at[q], down_g)
    own_sums = [begin(up_old, up_was, 11), begin(down_old, down_was, 12)]
    line_entered()
    gather_relay("cot", 1)
    square_relay(1, down_g)
    send_pre()
    own_late.wait()
    gather_own("late", 1)
    relay_rest("cot")
    own_early[0].wait()
    gather_own("early0", 1)
    gather_own("late", 0)
    own_up.wait()
    square_send(0, up_g.at[q], up_g)
    hops(mine, pre_relay, range(3, a))
    own_rest("late")
    square_relay(0, up_g)
    hops(mine, pre_relay, (1,))
    gather_own("early0", 0)
    gather_relay("late", 1, (0,))
    gather_relay("late", 1, (1,))
    hops(mine, pre_relay, (2,))
    hidden_grad_terms()
    own_early[1].wait()
    gather_own("early1", 0)
    gather_own("early1", 1)
    early_hidden()
    pre_grad()
    gather_relay("early0", 1)
    dg.start()
    relay_rest("late", (0,))
    relay_rest("late", (1,))
    square_rest(0, up_g)
    ig[0].start()
    gather_relay("early1", 1)
    own_rest("early0")
    ig[1].start()
    ig[0].relay(1, True)
    own_rest("early1")
    relay_rest("early0")
    late_terms()
    ig[0].relay(2, False)
    late_hidden()
    settled = len(sent)
    ig[1].relay(1, True)
    relay_rest("early1")
    lo[0].start()
    dg.relay()
    lo[1].start()
    ig[1].relay(2, False)
    gather_end("early0")
    ug[0].start()
    gather_end("early1")
    ug[1].start()
    send_late_pre()
    line_rest(ig[0])
    lo[0].relay(1, True)
    keep_own()
    lo[1].relay(1, True)
    line_rest(ig[1])
    lo[0].relay(2, False)
    ug[0].relay()
    ig[1].finish()
    ug[1].relay()
    line_rest(lo[0])
    ug[0].finish()
    ig[0].finish()
    lo[1].relay(2, False)
    line_rest(lo[1])
    down_finish()
    lo[0].finish()
    settle(settled)
    hops(mine, out_relay, (2,))
    hops(mine, out_relay, range(3, a))
    hops(mine, out_relay, (1,))
    ug[1].finish()
    lo[1].finish()
    hops(other, out_rest)

    settle(len(sent))


def store_body(*refs):
    n = len(refs) // 2
    sems = refs[2 * n]
    copies = [pltpu.make_async_copy(refs[k], refs[n + k], sems.at[k]) for k in range(n)]
    for copy in copies:
        copy.start()
    for copy in copies:
        copy.wait()


def store(results):
    n = len(results)
    return pl.pallas_call(
        store_body,
        out_shape=tuple(jax.ShapeDtypeStruct(r.shape, r.dtype) for r in results),
        in_specs=[pl.BlockSpec(memory_space=pltpu.VMEM)] * n,
        out_specs=[pl.BlockSpec(memory_space=pltpu.HBM)] * n,
        scratch_shapes=[pltpu.SemaphoreType.DMA((n,))],
        compiler_params=pltpu.CompilerParams(vmem_limit_bytes=16 * 1024 * 1024),
    )(*results)


def fused_body(late_input, up_weight, down_weight, early_input, early_pre, cotangent, up_sum, down_sum):
    a = lax.axis_size("fs") // 4
    side = 4
    rows, width = late_input.shape
    ff = up_weight.shape[1]
    tokens, hidden = rows * a, ff * side
    cut = width // 2
    V = pltpu.VMEM
    D = pltpu.SemaphoreType.DMA
    token_block = V((tokens, width), BF16)
    hidden_block = V((side, tokens, ff), BF16)
    line_block = V((2, a, rows, cut), BF16)
    scratch = (
        [token_block] * 2
        + [V((2, tokens, cut), BF16)]
        + [hidden_block, V((side, width, ff), BF16), V((side, ff, width), BF16)]
        + [hidden_block] * 8
        + [V((rows, hidden * a), BF16), V((2, 2, tokens, cut), F32)]
        + [line_block] * 6
        + [V((side, ff, width), BF16)] + [V((ff // 2, width), BF16)] * 2 + [V((ff, width), BF16)] * 2
        + [V((2, side, cut, ff), BF16)] + [V((2, cut // 2, ff), BF16)] * 2 + [V((2, cut, ff), BF16)] * 2
        + [D((6, 2, a)), D((6, 2, a)), D((2, 2, 3)), D((2, 2, 3)), D((2, a, 2)), D((2, a, 2)),
           D((2, a, 2)), D((2, a, 2)), D((2,)), D((2,)), D((2, 2, 2, a)), D((2, 2, 2, a)),
           D((2, 2, 6)), D((2, 2, 6)), D((13,))]
        + [V((width, ff), F32), V((ff, width), F32), pltpu.SemaphoreType.REGULAR((2,))]
    )
    flops = 12 * tokens * hidden * width
    results = pl.pallas_call(
        lambda *refs: fused(a, *refs),
        out_shape=(
            jax.ShapeDtypeStruct(early_pre.shape, BF16),
            jax.ShapeDtypeStruct(late_input.shape, BF16),
            jax.ShapeDtypeStruct(early_input.shape, BF16),
            jax.ShapeDtypeStruct(up_sum.shape, F32),
            jax.ShapeDtypeStruct(down_sum.shape, F32),
        ),
        in_specs=[pl.BlockSpec(memory_space=pltpu.HBM)] * 8,
        out_specs=[pl.BlockSpec(memory_space=pltpu.VMEM)] * 5,
        scratch_shapes=scratch,
        compiler_params=pltpu.CompilerParams(
            collective_id=0, has_side_effects=True, vmem_limit_bytes=48 * 1024 * 1024),
        cost_estimate=pl.CostEstimate(flops=flops, bytes_accessed=1 << 24, transcendentals=0),
    )(*[pltpu.with_memory_space_constraint(v, pltpu.HBM) for v in (
        late_input, up_weight, down_weight, early_input, early_pre, cotangent, up_sum, down_sum)])
    return store(results)


def contract_rows(left, right):
    return lax.dot_general(
        left, right, (((0,), (0,)), ((), ())), preferred_element_type=jnp.float32
    )


def contract_cols(left, right):
    return lax.dot_general(
        left, right, (((1,), (1,)), ((), ())), preferred_element_type=jnp.float32
    )


def body(late_input, up_weight, down_weight, early_input, early_pre, cotangent, up_sum, down_sum):
    up_gathered = lax.all_gather(up_weight, "fs", axis=1, tiled=True)
    down_gathered = lax.all_gather(down_weight, "fs", axis=0, tiled=True)
    pre_terms = jnp.dot(late_input, up_gathered, preferred_element_type=jnp.float32)
    pre_summed = lax.psum(pre_terms.astype(jnp.bfloat16), "tp")
    late_hidden = jnp.square(jax.nn.relu(pre_summed.astype(jnp.float32))).astype(jnp.bfloat16)
    early_float = early_pre.astype(jnp.float32)
    early_hidden = jnp.square(jax.nn.relu(early_float)).astype(jnp.bfloat16)
    late_out = jnp.dot(late_hidden, down_gathered, preferred_element_type=jnp.float32).astype(
        jnp.bfloat16
    )
    grad_terms = contract_cols(cotangent, down_gathered)
    hidden_grad = lax.psum(grad_terms.astype(jnp.bfloat16), "tp").astype(jnp.float32)
    pre_grad = (hidden_grad * 2.0 * jax.nn.relu(early_float)).astype(jnp.bfloat16)
    input_grad = contract_cols(pre_grad, up_gathered).astype(jnp.bfloat16)
    grad_local, hidden_local = (
        lax.all_to_all(pre_grad, "fs", split_axis=1, concat_axis=0, tiled=True),
        lax.all_to_all(early_hidden, "fs", split_axis=1, concat_axis=0, tiled=True),
    )
    rows = grad_local
    up_grad = contract_rows(lax.all_gather(early_input, "fs", axis=0, tiled=True), rows)
    up_total = up_sum + up_grad
    rows = hidden_local
    down_grad = contract_rows(rows, lax.all_gather(cotangent, "fs", axis=0, tiled=True))
    down_total = down_sum + down_grad
    return (pre_summed, late_out, input_grad, up_total, down_total)


def solution(mesh):
    in_specs = (
        P("fs", "tp"),
        P("tp", "fs"),
        P("fs", "tp"),
        P("fs", "tp"),
        P("fs", None),
        P("fs", "tp"),
        P("tp", "fs"),
        P("fs", "tp"),
    )
    out_specs = (P("fs", None), P("fs", "tp"), P("fs", "tp"), P("tp", "fs"), P("fs", "tp"))
    square_chips = mesh.shape["tp"] == 2 and mesh.shape["fs"] % 4 == 0 and mesh.shape["fs"] >= 8
    chosen = fused_body if square_chips else body
    return jax.shard_map(chosen, mesh=mesh, in_specs=in_specs, out_specs=out_specs, check_vma=False)
```

```python
from types import SimpleNamespace

import jax
import jax.numpy as jnp
from jax import lax
from jax.experimental import pallas as pl
from jax.experimental.pallas import tpu as pltpu
from jax.sharding import PartitionSpec as P

MESH = pl.DeviceIdType.MESH
F32 = jnp.float32
BF16 = jnp.bfloat16


def dot(left, right, lc, rc):
    return lax.dot_general(left, right, (((lc,), (rc,)), ((), ())), preferred_element_type=F32)


def square_relu(value):
    kept = jnp.maximum(value.astype(F32), 0.0)
    return (kept * kept).astype(BF16)


def fused(a, late_in, up_w, down_w, early_in, early_pre, cot, up_old, down_old,
          late_pre_o, lo_v, ig_v, up_v, down_v,
          cot_g, late_g, early_g, pre_g, up_g, down_g, gt_s, gt_r, pg, eh, lt_s, lt_r, lp, lh, lp_g,
          part, ig_s, ig_u, ig_d, lo_s, lo_u, lo_d,
          dg_s, dg_x, dg_y, dg_fx, dg_fy, ug_s, ug_x, ug_y, ug_fx, ug_fy,
          ag_ss, ag_rs, w_ss, w_rs, e_ss, e_rs, l_ss, l_rs, t_ss, t_rs, rl_ss, rl_rs, rq_ss, rq_rs,
          local_s, up_was, down_was, line_s):
    side = 4
    half_side = side // 2
    me = lax.axis_index("fs")
    t = lax.axis_index("tp")
    z = me // side
    q = lax.rem(me, side)
    y = q // 2
    x = lax.rem(q, 2)
    qx = y * 2 + (1 - x)
    qy = (1 - y) * 2 + x
    qd = side - 1 - q
    xn = (z * side + qx, t)
    yn = (z * side + qy, t)
    pn = (me, 1 - t)
    above = (lax.rem(me + side, a * side), t)
    below = (lax.rem(me + (a - 1) * side, a * side), t)
    rows = late_in.shape[0]
    ff = up_w.shape[1]
    width = late_in.shape[1]
    cut = width // 2
    last = a - 1
    middle = (z > 0) & (z < last)

    def begin(src, dst, k):
        copy = pltpu.make_async_copy(src, dst, local_s.at[k])
        copy.start()
        return copy

    def slot(j):
        return pl.ds(pl.multiple_of(j * rows, rows), rows)

    def slots(n):
        size = rows // n
        return lambda j, c: pl.ds(pl.multiple_of(j * rows + c * size, size), size)

    def columns(block, unit):
        return pl.ds(pl.multiple_of(block * unit, unit), unit)

    own_rows = slot(z)
    own_cot = begin(cot, cot_g.at[own_rows], 1)
    own_down = begin(down_w, down_g.at[q], 0)
    own_late = begin(late_in, late_g.at[own_rows], 3)
    own_early = [begin(early_in.at[:, pl.ds(c * cut, cut)], early_g.at[c, own_rows], 9 + c) for c in range(2)]
    own_up = begin(up_w, up_g.at[q], 2)
    own_pre = [
        begin(early_pre.at[:, pl.ds(pl.multiple_of((z * side + b) * ff, ff), ff)],
              pre_g.at[b, own_rows], 5 + b)
        for b in range(side)
    ]


    barrier = pltpu.get_barrier_semaphore()
    has_above = z < last
    has_below = z > 0

    def signal(semaphore, device):
        pl.semaphore_signal(semaphore, inc=1, device_id=device, device_id_type=MESH)

    for device in (xn, yn, pn):
        signal(barrier, device)
    pl.when(has_above)(lambda: signal(barrier, above))
    pl.when(has_below)(lambda: signal(barrier, below))
    pl.semaphore_wait(barrier, 3 + jnp.where(has_above, 1, 0) + jnp.where(has_below, 1, 0))

    def line_entered():
        pl.when(has_above)(lambda: pl.semaphore_wait(line_s.at[0], 1))
        pl.when(has_below)(lambda: signal(line_s.at[0], below))
        pl.when(has_below)(lambda: pl.semaphore_wait(line_s.at[1], 1))
        pl.when(has_above)(lambda: signal(line_s.at[1], above))

    sent = []

    def run(cond, go):
        if cond is None:
            go()
        else:
            pl.when(cond)(go)

    def rc(src, dst, ss, rs, device):
        return pltpu.make_async_remote_copy(
            src_ref=src, dst_ref=dst, send_sem=ss, recv_sem=rs, device_id=device, device_id_type=MESH)

    def send(src, dst, ss, rs, device, cond=None):
        copy = rc(src, dst, ss, rs, device)
        run(cond, copy.start)
        sent.append((cond, copy))

    def settle(count):
        for cond, copy in sent[:count]:
            run(cond, copy.wait_send)
        del sent[:count]

    def arrive(dst, ss, rs, cond=None):
        run(cond, rc(dst, dst, ss, rs, pn).wait_recv)

    gathers = {
        "cot": (0, 2, lambda j, c: cot_g.at[slots(2)(j, c)]),
        "late": (2, 2, lambda j, c: late_g.at[slots(2)(j, c)]),
        "early0": (4, 1, lambda j, c: early_g.at[0, slot(j)]),
        "early1": (5, 1, lambda j, c: early_g.at[1, slot(j)]),
    }

    def gather_own(name, depth=None):
        first, pieces, piece = gathers[name]
        for c in range(pieces):
            own = piece(z, c)
            for way, edge, device in ((0, z < last, above), (1, z > 0, below)):
                left = z if way == 0 else last - z
                cond = edge if depth is None else edge & (left == depth)
                send(own, own, ag_ss.at[first + c, way, 0], ag_rs.at[first + c, way, 1], device, cond)

    def gather_relay(name, d, some=None):
        if d >= last:
            return
        first, pieces, piece = gathers[name]
        for c in range(pieces) if some is None else some:
            for way, here, j, device in ((0, (z >= d) & (z < last), z - d, above),
                                         (1, (z + d < a) & (z > 0), z + d, below)):
                place = piece(jnp.clip(j, 0, last), c)
                arrive(place, ag_ss.at[first + c, way, 0], ag_rs.at[first + c, way, d], here)
                send(place, place, ag_ss.at[first + c, way, d], ag_rs.at[first + c, way, d + 1], device, here)

    def gather_end(name):
        first, pieces, piece = gathers[name]
        for d in range(1, a):
            for c in range(pieces):
                for way, here, j in ((0, z == last, z - d), (1, z == 0, z + d)):
                    place = piece(jnp.clip(j, 0, last), c)
                    arrive(place, ag_ss.at[first + c, way, 0], ag_rs.at[first + c, way, d], here)

    def half(ref, block, h):
        n = ref.shape[1] // 2
        return ref.at[block, pl.ds(h * n, n)]

    def half2(ref, h):
        n = ref.shape[0] // 2
        return ref.at[pl.ds(h * n, n)]

    def square_send(which, own, buf):
        for h in (0, 1):
            send(half2(own, h), half(buf, q, h), w_ss.at[which, 0, h], w_rs.at[which, 0, h], xn)
            send(half2(own, 1 - h), half(buf, q, 1 - h), w_ss.at[which, 1, 1 - h], w_rs.at[which, 1, 1 - h], yn)

    def square_relay(which, buf):
        arrive(half(buf, qx, 0), w_ss.at[which, 0, 0], w_rs.at[which, 0, 0])
        send(half(buf, qx, 0), half(buf, qx, 0), w_ss.at[which, 1, 2], w_rs.at[which, 1, 2], yn)
        arrive(half(buf, qy, 1), w_ss.at[which, 0, 0], w_rs.at[which, 1, 1])
        send(half(buf, qy, 1), half(buf, qy, 1), w_ss.at[which, 0, 2], w_rs.at[which, 0, 2], xn)

    def square_rest(which, buf):
        arrive(half(buf, qx, 1), w_ss.at[which, 0, 0], w_rs.at[which, 0, 1])
        arrive(half(buf, qy, 0), w_ss.at[which, 0, 0], w_rs.at[which, 1, 0])
        arrive(half(buf, qd, 0), w_ss.at[which, 0, 0], w_rs.at[which, 1, 2])
        arrive(half(buf, qd, 1), w_ss.at[which, 0, 0], w_rs.at[which, 0, 2])

    def square_sum(which, c, block, staged, first_x, first_y, fin_x, fin_y, was, out):
        n = staged.shape[1] // 2
        sems = lambda k: (rq_ss.at[which, c, k], rq_rs.at[which, c, k])
        wait = lambda dst, k: arrive(dst, *sems(k))

        def start():
            staged[qd] = block(qd).astype(BF16)
            send(half(staged, qd, 0), first_x, *sems(0), xn)
            send(half(staged, qd, 1), first_y, *sems(1), yn)
            staged[qx] = block(qx).astype(BF16)
            send(half(staged, qx, 0), half2(fin_x, 0), *sems(2), xn)
            staged[qy] = block(qy).astype(BF16)
            send(half(staged, qy, 1), half2(fin_y, 1), *sems(3), yn)

        def relay():
            wait(first_x, 0)
            staged[qy, 0:n] = (staged[qy, 0:n].astype(F32) + first_x[...].astype(F32)).astype(BF16)
            send(half(staged, qy, 0), half2(fin_y, 0), *sems(4), yn)
            wait(first_y, 1)
            staged[qx, n:2 * n] = (staged[qx, n:2 * n].astype(F32) + first_y[...].astype(F32)).astype(BF16)
            send(half(staged, qx, 1), half2(fin_x, 1), *sems(5), xn)

        def own():
            out[...] = block(q)

        def finish():
            wait(half2(fin_x, 0), 2)
            wait(half2(fin_y, 1), 3)
            wait(half2(fin_y, 0), 4)
            wait(half2(fin_x, 1), 5)
            out[...] = was[...] + (out[...] + (fin_x[...].astype(F32) + fin_y[...].astype(F32)))

        return SimpleNamespace(start=start, relay=relay, own=own, finish=finish)

    def line_sum(which, c, value, staged, from_u, from_d, out):
        own = part.at[which, c]

        def go(way, j, step, cond):
            buf, device = ((from_u, above), (from_d, below))[way]
            send(staged.at[c, j], buf.at[c, j], rl_ss.at[which, c, way, step], rl_rs.at[which, c, way, j], device, cond)

        def start():
            own[...] = value(c)
            for j in range(a):
                staged[c, j] = own[pl.ds(j * rows, rows)].astype(BF16)
            for step in range(last):
                go(0, last - step, step, z == 0)
                go(1, step, step, z == last)

        def relay(step, opening):
            if step >= last:
                return
            for way in range(2):
                if way == 0:
                    j, on, opens, buf = last + z - step, step >= z, z == step, from_u
                else:
                    j, on, opens, buf = step - (last - z), step >= last - z, last - z == step, from_d
                on = on & middle & (opens if opening else jnp.logical_not(opens))
                j = jnp.clip(j, 0, last)

                @pl.when(on)
                def _(j=j, buf=buf, way=way):
                    arrive(buf.at[c, j], rl_ss.at[which, 0, 0, 0], rl_rs.at[which, c, way, j])
                    staged[c, j] = (staged[c, j].astype(F32) + buf[c, j].astype(F32)).astype(BF16)

                go(way, j, step, on)

        def finish():
            @pl.when(z > 0)
            def _():
                arrive(from_u.at[c, z], rl_ss.at[which, 0, 0, 0], rl_rs.at[which, c, 0, z])
                own[own_rows] = own[own_rows] + from_u[c, z].astype(F32)

            @pl.when(z < last)
            def _():
                arrive(from_d.at[c, z], rl_ss.at[which, 0, 0, 0], rl_rs.at[which, c, 1, z])
                own[own_rows] = own[own_rows] + from_d[c, z].astype(F32)

            out[:, pl.ds(c * cut, cut)] = own[own_rows].astype(BF16)

        return SimpleNamespace(start=start, relay=relay, finish=finish)

    def hops(b_of, go, offsets=None):
        for o in range(1, a) if offsets is None else offsets:
            if o < a:
                zs = lax.rem(z - o + a, a)
                for u in range(half_side):
                    go(o, u, zs, b_of(u))

    mine = lambda u: t * half_side + u
    other = lambda u: (1 - t) * half_side + u

    def spread(source, target, ss, rs):
        for k in range(last, 0, -1):
            for o, cond in ((k, z + k <= last), (a - k, z >= k)):
                zd = lax.rem(z + o, a)
                for u in range(half_side):
                    b = mine(u)
                    send(source(zd, b), target(b), ss.at[0, o, u], rs.at[0, o, u], (zd * side + q, t), cond)

    def pre_relay(o, u, zs, b):
        place = pre_g.at[b, slot(zs)]
        arrive(place, e_ss.at[0, 0, 0], e_rs.at[0, o, u])
        send(place, place, e_ss.at[1, o, u], e_rs.at[1, o, u], pn)

    def pre_rest(o, u, zs, b):
        arrive(pre_g.at[b, slot(zs)], e_ss.at[0, 0, 0], e_rs.at[1, o, u])

    def out_relay(o, u, zs, b):
        place = lp_g.at[:, columns(zs * side + b, ff)]
        arrive(place, l_ss.at[0, 0, 0], l_rs.at[0, o, u])
        send(place, place, l_ss.at[1, o, u], l_rs.at[1, o, u], pn)
        late_pre_o[:, columns(zs * side + b, ff)] = place[...]

    def out_rest(o, u, zs, b):
        place = lp_g.at[:, columns(zs * side + b, ff)]
        arrive(place, l_ss.at[0, 0, 0], l_rs.at[1, o, u])
        late_pre_o[:, columns(zs * side + b, ff)] = place[...]

    def ig_value(c):
        return sum(dot(pg[b], up_g[b, pl.ds(c * cut, cut), :], 1, 1) for b in range(side))

    def lo_value(c):
        return sum(dot(lh[b], down_g[b, :, pl.ds(c * cut, cut)], 1, 0) for b in range(side))

    ig = [line_sum(0, c, ig_value, ig_s, ig_u, ig_d, ig_v) for c in range(2)]
    lo = [line_sum(1, c, lo_value, lo_s, lo_u, lo_d, lo_v) for c in range(2)]
    dg = square_sum(1, 0, lambda b: dot(eh[b], cot_g[...], 0, 0), dg_s, dg_x, dg_y, dg_fx, dg_fy, down_was, down_v)
    ug = [
        square_sum(0, c, lambda b, c=c: dot(early_g[c], pg[b], 0, 0), ug_s.at[c], ug_x.at[c], ug_y.at[c],
                   ug_fx.at[c], ug_fy.at[c], up_was.at[pl.ds(c * cut, cut)], up_v.at[pl.ds(c * cut, cut)])
        for c in range(2)
    ]

    def hidden_grad_terms():
        gather_end("cot")
        square_rest(1, down_g)

        @pl.loop(0, side)
        def _(b):
            gt_s[b] = dot(cot_g[...], down_g[b], 1, 1).astype(BF16)

        send(gt_s, gt_r, t_ss.at[0], t_rs.at[0], pn)

    def early_hidden():
        for copy in own_pre + own_sums:
            copy.wait()
        hops(other, pre_rest)

        @pl.loop(0, side)
        def _(b):
            eh[b] = square_relu(pre_g[b])

    def pre_grad():
        arrive(gt_r, t_ss.at[0], t_rs.at[0])

        @pl.loop(0, side)
        def _(b):
            hidden = gt_s[b].astype(F32) + gt_r[b].astype(F32)
            pg[b] = (hidden * 2.0 * jnp.maximum(pre_g[b].astype(F32), 0.0)).astype(BF16)

    def late_terms():
        gather_end("late")

        @pl.loop(0, side)
        def _(b):
            lt_s[b] = dot(late_g[...], up_g[b], 1, 0).astype(BF16)

        send(lt_s, lt_r, t_ss.at[1], t_rs.at[1], pn)

    def late_hidden():
        arrive(lt_r, t_ss.at[1], t_rs.at[1])

        @pl.loop(0, side)
        def _(b):
            pre = (lt_s[b].astype(F32) + lt_r[b].astype(F32)).astype(BF16)
            lp[b] = pre
            lh[b] = square_relu(pre)

    def send_pre():
        spread(lambda zd, b: early_pre.at[:, columns(zd * side + b, ff)],
               lambda b: pre_g.at[b, slot(z)], e_ss, e_rs)

    def send_late_pre():
        spread(lambda zd, b: lp.at[b, slot(zd)],
               lambda b: lp_g.at[:, columns(z * side + b, ff)], l_ss, l_rs)

    def keep_own():
        ug[0].own()
        ug[1].own()
        for b in range(side):
            late_pre_o[:, columns(z * side + b, ff)] = lp[b, slot(z)]

    def down_finish():
        dg.own()
        dg.finish()

    def relay_rest(name, some=None):
        for d in range(2, last):
            gather_relay(name, d, some)

    def own_rest(name):
        for d in range(2, last):
            gather_own(name, d)

    def line_rest(chain):
        chain.relay(2, True)
        for k in range(3, last):
            chain.relay(k, False)
            chain.relay(k, True)

    own_cot.wait()
    gather_own("cot")
    own_down.wait()
    square_send(1, down_g.at[q], down_g)
    own_sums = [begin(up_old, up_was, 11), begin(down_old, down_was, 12)]
    line_entered()
    gather_relay("cot", 1)
    square_relay(1, down_g)
    send_pre()
    own_late.wait()
    gather_own("late", 1)
    relay_rest("cot")
    own_early[0].wait()
    gather_own("early0", 1)
    gather_own("late", 0)
    own_up.wait()
    square_send(0, up_g.at[q], up_g)
    hops(mine, pre_relay, range(3, a))
    own_rest("late")
    square_relay(0, up_g)
    hops(mine, pre_relay, (1,))
    gather_own("early0", 0)
    gather_relay("late", 1, (0,))
    gather_relay("late", 1, (1,))
    hops(mine, pre_relay, (2,))
    hidden_grad_terms()
    own_early[1].wait()
    gather_own("early1", 0)
    gather_own("early1", 1)
    early_hidden()
    pre_grad()
    gather_relay("early0", 1)
    dg.start()
    relay_rest("late", (0,))
    relay_rest("late", (1,))
    square_rest(0, up_g)
    ig[0].start()
    gather_relay("early1", 1)
    own_rest("early0")
    ig[1].start()
    ig[0].relay(1, True)
    own_rest("early1")
    relay_rest("early0")
    late_terms()
    ig[0].relay(2, False)
    late_hidden()
    settled = len(sent)
    ig[1].relay(1, True)
    relay_rest("early1")
    lo[0].start()
    dg.relay()
    lo[1].start()
    ig[1].relay(2, False)
    gather_end("early0")
    ug[0].start()
    gather_end("early1")
    ug[1].start()
    send_late_pre()
    line_rest(ig[0])
    lo[0].relay(1, True)
    keep_own()
    lo[1].relay(1, True)
    line_rest(ig[1])
    lo[0].relay(2, False)
    ug[0].relay()
    ig[1].finish()
    ug[1].relay()
    line_rest(lo[0])
    ug[0].finish()
    ig[0].finish()
    lo[1].relay(2, False)
    line_rest(lo[1])
    down_finish()
    lo[0].finish()
    settle(settled)
    hops(mine, out_relay, (2,))
    hops(mine, out_relay, range(3, a))
    hops(mine, out_relay, (1,))
    settle(len(sent))
    ug[1].finish()
    lo[1].finish()
    hops(other, out_rest)

    settle(len(sent))


def store_body(*refs):
    n = len(refs) // 2
    sems = refs[2 * n]
    copies = [pltpu.make_async_copy(refs[k], refs[n + k], sems.at[k]) for k in range(n)]
    for copy in copies:
        copy.start()
    for copy in copies:
        copy.wait()


def store(results):
    n = len(results)
    return pl.pallas_call(
        store_body,
        out_shape=tuple(jax.ShapeDtypeStruct(r.shape, r.dtype) for r in results),
        in_specs=[pl.BlockSpec(memory_space=pltpu.VMEM)] * n,
        out_specs=[pl.BlockSpec(memory_space=pltpu.HBM)] * n,
        scratch_shapes=[pltpu.SemaphoreType.DMA((n,))],
        compiler_params=pltpu.CompilerParams(vmem_limit_bytes=16 * 1024 * 1024),
    )(*results)


def fused_body(late_input, up_weight, down_weight, early_input, early_pre, cotangent, up_sum, down_sum):
    a = lax.axis_size("fs") // 4
    side = 4
    rows, width = late_input.shape
    ff = up_weight.shape[1]
    tokens, hidden = rows * a, ff * side
    cut = width // 2
    V = pltpu.VMEM
    D = pltpu.SemaphoreType.DMA
    token_block = V((tokens, width), BF16)
    hidden_block = V((side, tokens, ff), BF16)
    line_block = V((2, a, rows, cut), BF16)
    scratch = (
        [token_block] * 2
        + [V((2, tokens, cut), BF16)]
        + [hidden_block, V((side, width, ff), BF16), V((side, ff, width), BF16)]
        + [hidden_block] * 8
        + [V((rows, hidden * a), BF16), V((2, 2, tokens, cut), F32)]
        + [line_block] * 6
        + [V((side, ff, width), BF16)] + [V((ff // 2, width), BF16)] * 2 + [V((ff, width), BF16)] * 2
        + [V((2, side, cut, ff), BF16)] + [V((2, cut // 2, ff), BF16)] * 2 + [V((2, cut, ff), BF16)] * 2
        + [D((6, 2, a)), D((6, 2, a)), D((2, 2, 3)), D((2, 2, 3)), D((2, a, 2)), D((2, a, 2)),
           D((2, a, 2)), D((2, a, 2)), D((2,)), D((2,)), D((2, 2, 2, a)), D((2, 2, 2, a)),
           D((2, 2, 6)), D((2, 2, 6)), D((13,))]
        + [V((width, ff), F32), V((ff, width), F32), pltpu.SemaphoreType.REGULAR((2,))]
    )
    flops = 12 * tokens * hidden * width
    results = pl.pallas_call(
        lambda *refs: fused(a, *refs),
        out_shape=(
            jax.ShapeDtypeStruct(early_pre.shape, BF16),
            jax.ShapeDtypeStruct(late_input.shape, BF16),
            jax.ShapeDtypeStruct(early_input.shape, BF16),
            jax.ShapeDtypeStruct(up_sum.shape, F32),
            jax.ShapeDtypeStruct(down_sum.shape, F32),
        ),
        in_specs=[pl.BlockSpec(memory_space=pltpu.HBM)] * 8,
        out_specs=[pl.BlockSpec(memory_space=pltpu.VMEM)] * 5,
        scratch_shapes=scratch,
        compiler_params=pltpu.CompilerParams(
            collective_id=0, has_side_effects=True, vmem_limit_bytes=48 * 1024 * 1024),
        cost_estimate=pl.CostEstimate(flops=flops, bytes_accessed=1 << 24, transcendentals=0),
    )(*[pltpu.with_memory_space_constraint(v, pltpu.HBM) for v in (
        late_input, up_weight, down_weight, early_input, early_pre, cotangent, up_sum, down_sum)])
    return store(results)


def contract_rows(left, right):
    return lax.dot_general(
        left, right, (((0,), (0,)), ((), ())), preferred_element_type=jnp.float32
    )


def contract_cols(left, right):
    return lax.dot_general(
        left, right, (((1,), (1,)), ((), ())), preferred_element_type=jnp.float32
    )


def body(late_input, up_weight, down_weight, early_input, early_pre, cotangent, up_sum, down_sum):
    up_gathered = lax.all_gather(up_weight, "fs", axis=1, tiled=True)
    down_gathered = lax.all_gather(down_weight, "fs", axis=0, tiled=True)
    pre_terms = jnp.dot(late_input, up_gathered, preferred_element_type=jnp.float32)
    pre_summed = lax.psum(pre_terms.astype(jnp.bfloat16), "tp")
    late_hidden = jnp.square(jax.nn.relu(pre_summed.astype(jnp.float32))).astype(jnp.bfloat16)
    early_float = early_pre.astype(jnp.float32)
    early_hidden = jnp.square(jax.nn.relu(early_float)).astype(jnp.bfloat16)
    late_out = jnp.dot(late_hidden, down_gathered, preferred_element_type=jnp.float32).astype(
        jnp.bfloat16
    )
    grad_terms = contract_cols(cotangent, down_gathered)
    hidden_grad = lax.psum(grad_terms.astype(jnp.bfloat16), "tp").astype(jnp.float32)
    pre_grad = (hidden_grad * 2.0 * jax.nn.relu(early_float)).astype(jnp.bfloat16)
    input_grad = contract_cols(pre_grad, up_gathered).astype(jnp.bfloat16)
    grad_local, hidden_local = (
        lax.all_to_all(pre_grad, "fs", split_axis=1, concat_axis=0, tiled=True),
        lax.all_to_all(early_hidden, "fs", split_axis=1, concat_axis=0, tiled=True),
    )
    rows = grad_local
    up_grad = contract_rows(lax.all_gather(early_input, "fs", axis=0, tiled=True), rows)
    up_total = up_sum + up_grad
    rows = hidden_local
    down_grad = contract_rows(rows, lax.all_gather(cotangent, "fs", axis=0, tiled=True))
    down_total = down_sum + down_grad
    return (pre_summed, late_out, input_grad, up_total, down_total)


def solution(mesh):
    in_specs = (
        P("fs", "tp"),
        P("tp", "fs"),
        P("fs", "tp"),
        P("fs", "tp"),
        P("fs", None),
        P("fs", "tp"),
        P("tp", "fs"),
        P("fs", "tp"),
    )
    out_specs = (P("fs", None), P("fs", "tp"), P("fs", "tp"), P("tp", "fs"), P("fs", "tp"))
    square_chips = mesh.shape["tp"] == 2 and mesh.shape["fs"] % 4 == 0 and mesh.shape["fs"] >= 8
    chosen = fused_body if square_chips else body
    return jax.shard_map(chosen, mesh=mesh, in_specs=in_specs, out_specs=out_specs, check_vma=False)
```
